32 devices in a mesh: sp: 16 (over z, y, core), tp: 2 (over x).
Axes of the slice: x: 2, y: 2, z: 4, core: 2. Of those that a mesh axis runs over, the one named last changes fastest.
Arguments:
- target: bfloat16 [2048, 2048], P('sp'), may hold values from -0.375 to 0.375
- source: bfloat16 [4096, 2048], P(('sp', 'tp')), may hold values from -0.375 to 0.375
- target_gain: float32 [2048], replicated, may hold values from 0.3 to 12
- source_gain: float32 [2048], replicated, may hold values from 0.3 to 12
- w_query: bfloat16 [2048, 1024], P(None, 'tp'), may hold values from -0.125 to 0.125
- w_key: bfloat16 [2048, 256], replicated, may hold values from -0.125 to 0.125
- w_value: bfloat16 [2048, 256], replicated, may hold values from -0.125 to 0.125
- attended: bfloat16 [2048, 1024], P('sp', 'tp'), may hold values from -6 to 6
- d_attended: bfloat16 [2048, 1024], P('sp', 'tp'), may hold values from -24 to 24
Outputs:
- d_target: bfloat16 [2048, 2048], P('sp')
- d_source: float32 [4096, 2048], P(('sp', 'tp'))
- d_w_query: float32 [2048, 1024], P('sp', 'tp')
The draws below stay inside these ranges and needn't reach their ends.
All inputs are finite; a program needn't handle non-finite values.
Results may differ from the reference program's by a relative error of at most 0.02.
The reference program's roundings to bfloat16 on the way count: a program that leaves them out, or rounds other values in their place, can miss the bound.
Values may be sent and summed in bfloat16 or wider, within the bound.
A program may use at most 64 MiB of HBM per device.

```python
import jax
import jax.numpy as jnp
from jax import lax

D = 2048
HQ = 8
KVH = 2
HD = 128
TT = 2048
SS = 4096


def gain_law(key):
    return jax.random.uniform(key, (D,), jnp.float32, 0.3, 1.7)


def draw_target_gain(key, part):
    return gain_law(jax.random.fold_in(key, 11))


def draw_source_gain(key, part):
    return gain_law(jax.random.fold_in(key, 23))


def level_of(rng, extent, pieces, least, largest):
    factor_of = 1.0
    for position, parts in pieces:
        heights = jax.random.uniform(jax.random.fold_in(jax.random.fold_in(rng, 6), position), (parts,), jnp.float32, least / len(pieces), largest / len(pieces))
        factor_of = factor_of * jnp.repeat(jnp.exp(heights), extent[position] // parts).reshape((-1,) + (1,) * (len(extent) - 1 - position))
    return factor_of


def gaussian(key, dims, deviation, most, shards=(), held_as=jnp.bfloat16):
    loudness = level_of(key, dims, shards, -0.22, 0.18) if shards else 1.0
    array = jax.random.normal(key, dims, jnp.float32) * deviation * loudness
    return jnp.minimum(jnp.maximum(array, -most), most).astype(held_as)


def setup_inputs(seed: int = 0) -> dict:
    key_of = jax.random.split(jax.random.key(seed), 10)
    target = gaussian(key_of[0], (TT, D), 0.0625, 0.375, ((0, 16),))
    source = gaussian(key_of[1], (SS, D), 0.0625, 0.375, ((0, 32),))
    target_gain = draw_target_gain(jax.random.fold_in(key_of[9], 71), 0)
    source_gain = draw_source_gain(jax.random.fold_in(key_of[9], 71), 0)
    w_query = gaussian(key_of[4], (D, HQ * HD), D ** -0.5, 0.125, ((1, 2),))
    w_key = gaussian(key_of[5], (D, KVH * HD), D ** -0.5, 0.125)
    w_value = gaussian(key_of[6], (D, KVH * HD), D ** -0.5, 0.125)
    attended = gaussian(key_of[7], (TT, HQ * HD), 1.0, 6.0, ((0, 16), (1, 2)))
    d_attended = gaussian(key_of[8], (TT, HQ * HD), 4.0, 24.0, ((0, 16), (1, 2)))
    return {"target": target, "source": source, "target_gain": target_gain, "source_gain": source_gain, "w_query": w_query, "w_key": w_key, "w_value": w_value, "attended": attended, "d_attended": d_attended}


EPS = 1e-06

def norm_rows(matrix, gain_vector):
    widened = matrix.astype(jnp.float32)
    inverse = lax.rsqrt(lax.optimization_barrier(jnp.mean(widened * widened, axis=-1, keepdims=True)) + EPS)
    return widened * inverse * gain_vector

def norm_back(matrix, gain_vector, cotangent):
    _, pullback = jax.vjp(lambda values: norm_rows(values, gain_vector), matrix.astype(jnp.float32))
    return pullback(cotangent)[0]

def block_count(row_count, most_rows):
    number = 1
    while row_count % (number * 2) == 0 and row_count // number > most_rows:
        number = number * 2
    return number

def reference(target, source, target_gain, source_gain, w_query, w_key, w_value, attended, d_attended):
    scaling = HD ** (-0.5)
    group_size = HQ // KVH
    normed_target = norm_rows(target, target_gain).astype(jnp.bfloat16)
    normed_source = norm_rows(source, source_gain).astype(jnp.bfloat16)
    query = jnp.dot(normed_target, w_query, preferred_element_type=jnp.float32).astype(jnp.bfloat16)
    key = jnp.dot(normed_source, w_key, preferred_element_type=jnp.float32).astype(jnp.bfloat16)
    value = jnp.dot(normed_source, w_value, preferred_element_type=jnp.float32).astype(jnp.bfloat16)
    target_total = query.shape[0]
    source_total = key.shape[0]
    delta = lax.optimization_barrier(jnp.sum(d_attended.astype(jnp.float32).reshape(target_total, HQ, HD) * attended.astype(jnp.float32).reshape(target_total, HQ, HD), axis=-1)).astype(jnp.bfloat16)
    number = block_count(target_total, 512)
    block_rows = target_total // number

    def one_head(head_index):
        kv_index = head_index // group_size
        query_head = lax.dynamic_slice_in_dim(query, head_index * HD, HD, 1)
        key_head = lax.dynamic_slice_in_dim(key, kv_index * HD, HD, 1)
        value_head = lax.dynamic_slice_in_dim(value, kv_index * HD, HD, 1)
        grad_head = lax.dynamic_slice_in_dim(d_attended, head_index * HD, HD, 1)
        delta_head = lax.dynamic_slice_in_dim(delta, head_index, 1, 1)[:, 0]
        query_blocks = query_head.reshape(number, block_rows, HD)
        grad_blocks = grad_head.reshape(number, block_rows, HD)
        delta_blocks = delta_head.reshape(number, block_rows)

        def totals_of(queries):
            scores = jnp.dot(queries, key_head.T, preferred_element_type=jnp.float32) * scaling
            maxima = lax.optimization_barrier(jnp.max(scores, axis=-1))
            return maxima + jnp.log(lax.optimization_barrier(jnp.sum(jnp.exp(scores - maxima[:, None]), axis=-1)))
        log_total = lax.map(totals_of, query_blocks)

        def grad_step(carried, blocks):
            queries, cotangent, totals, delta_rows = blocks
            scores = jnp.dot(queries, key_head.T, preferred_element_type=jnp.float32) * scaling
            weights = jnp.exp(scores - totals[:, None])
            d_weights = jnp.dot(cotangent, value_head.T, preferred_element_type=jnp.float32)
            d_scores = (weights * (d_weights - delta_rows.astype(jnp.float32)[:, None])).astype(jnp.bfloat16)
            query_grad = jnp.dot(d_scores, key_head, preferred_element_type=jnp.float32) * scaling
            key_acc = carried[0] + jnp.dot(d_scores.T, queries, preferred_element_type=jnp.float32) * scaling
            value_acc = carried[1] + jnp.dot(weights.astype(jnp.bfloat16).T, cotangent, preferred_element_type=jnp.float32)
            return ((key_acc, value_acc), query_grad)
        start_state = (jnp.zeros((source_total, HD), jnp.float32), jnp.zeros((source_total, HD), jnp.float32))
        (key_acc, value_acc), query_grads = lax.scan(grad_step, start_state, (query_blocks, grad_blocks, log_total, delta_blocks))
        return (key_acc, value_acc, query_grads.reshape(target_total, HD))
    key_grads, value_grads, query_grads = lax.map(one_head, jnp.arange(HQ, dtype=jnp.int32))
    d_key = key_grads.reshape(KVH, group_size, source_total, HD).sum(axis=1)
    d_value = value_grads.reshape(KVH, group_size, source_total, HD).sum(axis=1)
    d_key_b = d_key.transpose(1, 0, 2).reshape(source_total, KVH * HD).astype(jnp.bfloat16)
    d_value_b = d_value.transpose(1, 0, 2).reshape(source_total, KVH * HD).astype(jnp.bfloat16)
    d_query_b = query_grads.transpose(1, 0, 2).reshape(target_total, HQ * HD).astype(jnp.bfloat16)
    d_w_query = jnp.dot(normed_target.T, d_query_b, preferred_element_type=jnp.float32)
    d_normed_target = jnp.dot(d_query_b, w_query.T, preferred_element_type=jnp.float32)
    d_target = norm_back(target, target_gain, d_normed_target).astype(jnp.bfloat16)
    d_normed_source = jnp.dot(d_key_b, w_key.T, preferred_element_type=jnp.float32) + jnp.dot(d_value_b, w_value.T, preferred_element_type=jnp.float32)
    d_source = norm_back(source, source_gain, d_normed_source)
    return (d_target, d_source, d_w_query)
```

```python
import functools

import jax
import jax.numpy as jnp
from jax import lax
from jax.experimental import pallas as pl
from jax.experimental.pallas import tpu as pltpu
from jax.sharding import PartitionSpec as P

KVH = 2
HD = 128
EPS = 1e-06
GROUP = 4
MESH = pl.DeviceIdType.MESH
F32 = jnp.float32
BF16 = jnp.bfloat16

NT_DIMS = (((1,), (1,)), ((), ()))


def dot_nn(a, b):
    return jnp.dot(a, b, preferred_element_type=F32)


def dot_nt(a, b):
    return lax.dot_general(a, b, NT_DIMS, preferred_element_type=F32)


def inverse_rms(x):
    return lax.rsqrt(jnp.mean(x * x, axis=-1, keepdims=True) + EPS)


def norm_back(x, gain, cotangent):
    inv = inverse_rms(x)
    gc = cotangent * gain
    inner = jnp.mean(x * gc, axis=-1, keepdims=True)
    return inv * gc - x * (inv * inv * inv * inner)


def kernel(
    sp_size,
    tp_size,
    target_h,
    source_h,
    tgain_h,
    sgain_h,
    wq_h,
    wk_h,
    wv_h,
    att_h,
    dout_h,
    dtarget,
    dsource,
    dwq,
    target,
    source,
    tgain,
    sgain,
    wq,
    wk,
    wv,
    att,
    ktg,
    kvown,
    kvg,
    qg,
    og,
    delta,
    ntt,
    nttg,
    probs,
    prods,
    cstat,
    stat,
    dks,
    dkg,
    dqacc,
    dqs,
    dqr,
    dqg,
    rets,
    ret,
    dnb,
    dkacc,
    dws,
    dwg,
    tkv_s,
    tkv_r,
    lkv_s,
    lkv_r,
    in_s,
    in_r,
    nt_s,
    nt_r,
    st_s,
    st_r,
    dk_s,
    dk_r,
    dq_s,
    dq_r,
    ag_s,
    ag_r,
    rt_s,
    rt_r,
    dn_s,
    dn_r,
    dw_s,
    dw_r,
    ld_s,
):
    outer = sp_size // GROUP
    rows = target.shape[0]
    width = wq.shape[1]
    heads = width // HD
    own_rows = source.shape[0]
    block = own_rows * tp_size
    group_rows = GROUP * rows
    scaling = HD ** (-0.5)
    sp = lax.axis_index("sp")
    t = lax.axis_index("tp")
    z = sp // GROUP
    g = sp % GROUP
    per_kv = tp_size // KVH

    def tp_peer(o):
        return lax.rem(t + o, tp_size)

    def g_peer(o):
        return lax.rem(g + o, GROUP)

    def z_peer(o):
        return lax.rem(z + o, outer)

    def to_tp(p):
        return {"sp": sp, "tp": p}

    def to_g(p):
        return {"sp": z * GROUP + p, "tp": t}

    def to_z(p):
        return {"sp": p * GROUP + g, "tp": t}

    def copy(src, dst, ssem, rsem, dev):
        return pltpu.make_async_remote_copy(
            src_ref=src, dst_ref=dst, send_sem=ssem, recv_sem=rsem, device_id=dev, device_id_type=MESH
        )

    ga = g + 1 - 2 * lax.rem(g, 2)
    gb = lax.rem(g + 2, GROUP)
    gc = lax.rem(ga + 2, GROUP)
    parts = wq_parts(heads)
    part_heads = heads // parts
    part_width = width // parts

    loads = [
        pltpu.make_async_copy(src, dst, ld_s.at[n])
        for n, (src, dst) in enumerate(
            (
                (dout_h, og.at[g]),
                (source_h, source),
                (sgain_h, sgain),
                (wk_h, wk),
                (wv_h, wv),
                (target_h, target),
                (tgain_h, tgain),
                (wq_h, wq),
                (att_h, att),
            )
        )
    ]
    for load in loads:
        load.start()

    barrier = pltpu.get_barrier_semaphore()
    for o in range(1, tp_size):
        pl.semaphore_signal(barrier, inc=1, device_id=to_tp(tp_peer(o)), device_id_type=MESH)
    for o in range(1, GROUP):
        pl.semaphore_signal(barrier, inc=1, device_id=to_g(g_peer(o)), device_id_type=MESH)
    for o in range(1, outer):
        pl.semaphore_signal(barrier, inc=1, device_id=to_z(z_peer(o)), device_id_type=MESH)
    pl.semaphore_wait(barrier, tp_size + GROUP + outer - 3)

    def group_copy(k, way, slot):
        ref = (og, qg, delta)[k].at[slot]
        return copy(ref, ref, in_s.at[k, way], in_r.at[k, slot], to_g((ga, gb, ga)[way]))

    def send_own(k):
        group_copy(k, 1, g).start()
        group_copy(k, 0, g).start()

    def forward(k):
        group_copy(k, 1, gb).wait_recv()
        group_copy(k, 2, gb).start()

    def columns_copy(p, slot):
        return copy(ntt.at[:, p], nttg.at[slot], nt_s.at[p], nt_r.at[slot], to_g(p))

    loads[0].wait()
    send_own(0)
    for n in range(1, 5):
        loads[n].wait()

    s32 = source[...].astype(F32)
    ns = (s32 * inverse_rms(s32) * sgain[...]).astype(BF16)
    keys = dot_nn(ns, wk[...]).astype(BF16)
    values = dot_nn(ns, wv[...]).astype(BF16)
    for c in range(KVH):
        kvown[c, :, 0:HD] = keys[:, c * HD : (c + 1) * HD]
        kvown[c, :, HD : 2 * HD] = values[:, c * HD : (c + 1) * HD]

    def tkv(p, slot):
        return copy(kvown.at[p // per_kv], kvg.at[z, slot], tkv_s.at[p], tkv_r.at[slot], to_tp(p))

    def lkv(p, zslot, tslot):
        return copy(
            kvg.at[z, tslot], kvg.at[zslot, tslot], lkv_s.at[p, tslot], lkv_r.at[zslot, tslot], to_z(p)
        )

    for o in range(1, tp_size):
        tkv(tp_peer(o), t).start()
    kvg[z, t] = kvown[t // per_kv]
    for o in range(1, outer):
        lkv(z_peer(o), z, t).start()

    for n in range(5, 9):
        loads[n].wait()
    t32 = target[...].astype(F32)
    nt32 = t32 * inverse_rms(t32) * tgain[...]
    qg[g] = dot_nn(nt32.astype(BF16), wq[...]).astype(BF16)
    send_own(1)
    prod = (og[g].astype(F32) * att[...].astype(F32)).T
    drows = [jnp.sum(prod[h * HD : (h + 1) * HD], axis=0, keepdims=True) for h in range(heads)]
    drows.append(jnp.zeros((8 - heads, rows), F32))
    delta[g] = jnp.concatenate(drows, axis=0).astype(BF16).astype(F32)
    send_own(2)
    for o in range(1, tp_size):
        p = tp_peer(o)
        tkv(t, p).wait_recv()
        for oz in range(1, outer):
            lkv(z_peer(oz), z, p).start()
    forward(0)
    forward(1)
    forward(2)
    ntt[...] = nt32.T.astype(BF16).reshape(ntt.shape)
    for p in (gc, gb, ga):
        columns_copy(p, g).start()
    nttg[g] = ntt[:, g]
    for p in (ga, gc):
        group_copy(1, 0, p).wait_recv()

    def columns(ref, h):
        return ref[:, :, h * HD : (h + 1) * HD].reshape(group_rows, HD)

    def first(o, _):
        zc = lax.rem(z + outer - o, outer)

        @pl.when(o > 0)
        def _():
            for ts in range(tp_size):
                lkv(zc, zc, ts).wait_recv()

        kb = kvg[zc, :, :, 0:HD].reshape(block, HD)
        ktg[zc] = kb.astype(F32).T.astype(BF16)
        for h in range(heads):
            s = dot_nt(kb, columns(qg, h)) * scaling
            m = jnp.max(s, axis=0, keepdims=True)
            e = jnp.exp(s - m)
            probs[zc, h] = e
            cstat[zc, h : h + 1, :] = m
            cstat[zc, 8 + h : 9 + h, :] = jnp.sum(e, axis=0, keepdims=True)
        return 0

    lax.fori_loop(0, outer, first, 0)

    m_all = cstat[:, 0:heads, :]
    m_loc = jnp.max(m_all, axis=0)
    l_loc = jnp.sum(cstat[:, 8 : 8 + heads, :] * jnp.exp(m_all - m_loc[None]), axis=0)
    stat[g, 0:heads, :] = m_loc
    stat[g, 8 : 8 + heads, :] = l_loc
    if heads < 8:
        stat[g, heads:8, :] = jnp.zeros((8 - heads, group_rows), F32)
        stat[g, 8 + heads : 16, :] = jnp.zeros((8 - heads, group_rows), F32)

    def stat_copy(p, slot):
        return copy(stat.at[g], stat.at[slot], st_s.at[p], st_r.at[slot], to_g(p))

    for o in range(1, GROUP):
        stat_copy(g_peer(o), g).start()
    for k in (0, 2):
        for p in (ga, gc):
            group_copy(k, 0, p).wait_recv()

    def middle(zc, _):
        vb = kvg[zc, :, :, HD : 2 * HD].reshape(block, HD)
        for h in range(heads):
            drow = jnp.concatenate([delta[i, h : h + 1, :] for i in range(GROUP)], axis=1)
            prods[zc, h] = probs[zc, h] * (dot_nt(vb, columns(og, h)) - drow)
        return 0

    lax.fori_loop(0, outer, middle, 0)
    for o in range(1, GROUP):
        p = g_peer(o)
        stat_copy(p, p).wait_recv()
    m_g = jnp.max(stat[:, 0:heads, :], axis=0)
    l_g = jnp.sum(stat[:, 8 : 8 + heads, :] * jnp.exp(stat[:, 0:heads, :] - m_g[None]), axis=0)
    log_total = m_g + jnp.log(l_g)
    dqacc[...] = jnp.zeros_like(dqacc)

    def dk_copy(p, slot):
        return copy(dks.at[p], dkg.at[slot], dk_s.at[p], dk_r.at[slot], to_z(p))

    def dq_copy(k, p, slot):
        return copy(dqs.at[k, p], dqr.at[k, slot], dq_s.at[k, p], dq_r.at[k, slot], to_g(p))

    for k in range(parts):

        def second(o, _):
            zc = lax.rem(z + 1 + o, outer)
            kbt = ktg[zc]
            dk = jnp.zeros((block, HD), F32)
            dv = jnp.zeros((block, HD), F32)
            for h in range(k * part_heads, (k + 1) * part_heads):
                qh = columns(qg, h)
                oh = columns(og, h)
                factor = jnp.exp(cstat[zc, h : h + 1, :] - log_total[h : h + 1, :])
                w = probs[zc, h] * factor
                ds = (prods[zc, h] * factor).astype(BF16)
                dk = dk + dot_nn(ds, qh)
                dv = dv + dot_nn(w.astype(BF16), oh)
                dqacc[h] += dot_nn(kbt, ds)
            dk = dk * scaling
            if k > 0:
                dk = dk + dkacc[zc, :, 0:HD]
                dv = dv + dkacc[zc, :, HD : 2 * HD]
            dkacc[zc, :, 0:HD] = dk
            dkacc[zc, :, HD : 2 * HD] = dv
            if k == parts - 1:

                @pl.when(o < outer - 1)
                def _():
                    dks[zc, :, 0:HD] = dk.astype(BF16)
                    dks[zc, :, HD : 2 * HD] = dv.astype(BF16)
                    dk_copy(zc, z).start()

            return 0

        lax.fori_loop(0, outer, second, 0)

        for i in range(GROUP):
            for h in range(part_heads):
                dqs[k, i, h * HD : (h + 1) * HD] = (
                    dqacc[k * part_heads + h, :, i * rows : (i + 1) * rows] * scaling
                ).astype(BF16)
        for p in (gc, gb, ga):
            dq_copy(k, p, g).start()

    def ag_copy(k, way, slot):
        ref = dqg.at[k, slot]
        return copy(ref, ref, ag_s.at[k, way], ag_r.at[k, slot], to_g((ga, gb, ga)[way]))

    dn_term = jnp.zeros((rows, wq.shape[0]), F32)
    for k in range(parts):
        dq_sum = dqs[k, g].astype(F32)
        for p in (ga, gb, gc):
            dq_copy(k, p, p).wait_recv()
            dq_sum = dq_sum + dqr[k, p].astype(F32)
        dqg[k, g] = dq_sum.T.astype(BF16)
        ag_copy(k, 1, g).start()
        ag_copy(k, 0, g).start()

    def dn_copy(p, slot):
        return copy(dnb.at[t], dnb.at[slot], dn_s.at[p], dn_r.at[slot], to_tp(p))

    for k in range(parts):
        dn_term = dn_term + dot_nt(dqg[k, g], wq[:, k * part_width : (k + 1) * part_width])
    dnb[t] = dn_term.astype(BF16)
    for o in range(1, tp_size):
        dn_copy(tp_peer(o), t).start()
    for k in range(parts):
        ag_copy(k, 1, gb).wait_recv()
        ag_copy(k, 2, gb).start()

    def dw_copy(k, p, slot):
        return copy(dws.at[k, p], dwg.at[k, slot], dw_s.at[k, p], dw_r.at[k, slot], to_z(p))

    depth = ntt.shape[2]

    def normed_columns(i):
        return nttg[i].reshape(outer * depth, rows)

    for p in (ga, gb, gc):
        columns_copy(p, p).wait_recv()
    for k in range(parts):
        term = dot_nn(normed_columns(g), dqg[k, g]) + dot_nn(normed_columns(gb), dqg[k, gb])
        for p in (ga, gc):
            ag_copy(k, 0, p).wait_recv()
            term = term + dot_nn(normed_columns(p), dqg[k, p])
        dws[k] = term.astype(BF16).reshape(dws.shape[1:])
        for o in range(1, outer):
            dw_copy(k, z_peer(o), z).start()

    for o in range(1, outer):
        p = z_peer(o)
        dk_copy(p, p).wait_recv()
    total = dkacc[z]
    for o in range(1, outer):
        total = total + dkg[z_peer(o)].astype(F32)
    rets[...] = total.astype(BF16).reshape(rets.shape)

    def ret_copy(p, slot):
        return copy(rets.at[p], ret.at[slot], rt_s.at[p], rt_r.at[slot], to_tp(p))

    for o in range(1, tp_size):
        ret_copy(tp_peer(o), t).start()
    ret[t] = rets[t]

    for o in range(1, tp_size):
        p = tp_peer(o)
        dn_copy(p, p).wait_recv()
    dn = dnb[0].astype(F32)
    for k in range(1, tp_size):
        dn = dn + dnb[k].astype(F32)
    dtarget[...] = norm_back(target[...].astype(F32), tgain[...], dn).astype(BF16)


    for o in range(1, tp_size):
        p = tp_peer(o)
        ret_copy(p, p).wait_recv()
    dns = jnp.zeros(source.shape, F32)
    for c in range(KVH):
        part = ret[c * per_kv].astype(F32)
        for k in range(1, per_kv):
            part = part + ret[c * per_kv + k].astype(F32)
        part = part.astype(BF16)
        dns = dns + dot_nt(part[:, 0:HD], wk[:, c * HD : (c + 1) * HD])
        dns = dns + dot_nt(part[:, HD : 2 * HD], wv[:, c * HD : (c + 1) * HD])
    dsource[...] = norm_back(source[...].astype(F32), sgain[...], dns)


    for k in range(parts):
        dw_total = dws[k, z].astype(F32)
        for o in range(1, outer):
            p = z_peer(o)
            dw_copy(k, p, p).wait_recv()
            dw_total = dw_total + dwg[k, p].astype(F32)
        dwq[:, k * part_width : (k + 1) * part_width] = dw_total

    for o in range(1, tp_size):
        p = tp_peer(o)
        tkv(p, t).wait_send()
        ret_copy(p, t).wait_send()
        dn_copy(p, t).wait_send()
    for k in range(3):
        group_copy(k, 0, g).wait_send()
        group_copy(k, 1, g).wait_send()
        group_copy(k, 2, gb).wait_send()
    for p in (ga, gb, gc):
        columns_copy(p, g).wait_send()
        stat_copy(p, g).wait_send()
        for k in range(parts):
            dq_copy(k, p, g).wait_send()
    for k in range(parts):
        ag_copy(k, 0, g).wait_send()
        ag_copy(k, 1, g).wait_send()
        ag_copy(k, 2, gb).wait_send()
    for o in range(1, outer):
        p = z_peer(o)
        for ts in range(tp_size):
            lkv(p, z, ts).wait_send()
        dk_copy(p, z).wait_send()
        for k in range(parts):
            dw_copy(k, p, z).wait_send()


def wq_parts(heads):
    return 2 if heads % 2 == 0 else 1


def local(target, source, target_gain, source_gain, w_query, w_key, w_value, attended, d_attended):
    sp_size = lax.axis_size("sp")
    tp_size = lax.axis_size("tp")
    outer = sp_size // GROUP
    rows, d = target.shape
    own_rows = source.shape[0]
    block = own_rows * tp_size
    width = w_query.shape[1]
    heads = width // HD
    depth = d // sp_size
    group_rows = GROUP * rows
    vmem = pltpu.VMEM
    dma = pltpu.SemaphoreType.DMA
    parts = wq_parts(heads)
    part_width = width // parts
    scratch = [
        vmem((rows, d), BF16),
        vmem((own_rows, d), BF16),
        vmem((1, d), F32),
        vmem((1, d), F32),
        vmem((d, width), BF16),
        vmem(w_key.shape, BF16),
        vmem(w_value.shape, BF16),
        vmem((rows, width), BF16),
        vmem((outer, HD, block), BF16),
        vmem((KVH, own_rows, 2 * HD), BF16),
        vmem((outer, tp_size, own_rows, 2 * HD), BF16),
        vmem((GROUP, rows, width), BF16),
        vmem((GROUP, rows, width), BF16),
        vmem((GROUP, 8, rows), F32),
        vmem((outer, GROUP, depth, rows), BF16),
        vmem((GROUP, outer, depth, rows), BF16),
        vmem((outer, heads, block, group_rows), F32),
        vmem((outer, heads, block, group_rows), F32),
        vmem((outer, 16, group_rows), F32),
        vmem((GROUP, 16, group_rows), F32),
        vmem((outer, block, 2 * HD), BF16),
        vmem((outer, block, 2 * HD), BF16),
        vmem((heads, HD, group_rows), F32),
        vmem((parts, GROUP, part_width, rows), BF16),
        vmem((parts, GROUP, part_width, rows), BF16),
        vmem((parts, GROUP, rows, part_width), BF16),
        vmem((tp_size, own_rows, 2 * HD), BF16),
        vmem((tp_size, own_rows, 2 * HD), BF16),
        vmem((tp_size, rows, d), BF16),
        vmem((outer, block, 2 * HD), F32),
        vmem((parts, outer, depth, part_width), BF16),
        vmem((parts, outer, depth, part_width), BF16),
    ]
    sems = [
        dma((tp_size,)),
        dma((tp_size,)),
        dma((outer, tp_size)),
        dma((outer, tp_size)),
        dma((3, 3)),
        dma((3, GROUP)),
        dma((GROUP,)),
        dma((GROUP,)),
        dma((GROUP,)),
        dma((GROUP,)),
        dma((outer,)),
        dma((outer,)),
        dma((parts, GROUP)),
        dma((parts, GROUP)),
        dma((parts, 3)),
        dma((parts, GROUP)),
        dma((tp_size,)),
        dma((tp_size,)),
        dma((tp_size,)),
        dma((tp_size,)),
        dma((parts, outer)),
        dma((parts, outer)),
        dma((9,)),
    ]
    spec = pl.BlockSpec(memory_space=pl.ANY)
    held = pl.pallas_call(
        functools.partial(kernel, sp_size, tp_size),
        out_shape=(
            pltpu.VMEM((rows, d), BF16),
            pltpu.VMEM((own_rows, d), F32),
            pltpu.VMEM((depth, width), F32),
        ),
        in_specs=[spec] * 9,
        out_specs=(pl.BlockSpec(memory_space=pltpu.VMEM),) * 3,
        scratch_shapes=scratch + sems,
        compiler_params=pltpu.CompilerParams(
            collective_id=0, has_side_effects=True, vmem_limit_bytes=60000 * 1024
        ),
    )(
        *[
            pltpu.with_memory_space_constraint(x, pltpu.HBM)
            for x in (
                target,
                source,
                target_gain.reshape(1, d),
                source_gain.reshape(1, d),
                w_query,
                w_key,
                w_value,
                attended,
                d_attended,
            )
        ]
    )

    return pl.pallas_call(
        store_kernel,
        out_shape=(
            jax.ShapeDtypeStruct((rows, d), BF16),
            jax.ShapeDtypeStruct((own_rows, d), F32),
            jax.ShapeDtypeStruct((depth, width), F32),
        ),
        in_specs=[pl.BlockSpec(memory_space=pltpu.VMEM)] * 3,
        out_specs=(spec,) * 3,
        scratch_shapes=[dma((3,))],
    )(*[pltpu.with_memory_space_constraint(x, pltpu.VMEM) for x in held])


def store_kernel(a, b, c, a_h, b_h, c_h, sem):
    stores = [
        pltpu.make_async_copy(src, dst, sem.at[n])
        for n, (src, dst) in enumerate(((a, a_h), (b, b_h), (c, c_h)))
    ]
    for store in stores:
        store.start()
    for store in stores:
        store.wait()


def solution(mesh):
    return jax.shard_map(
        local,
        mesh=mesh,
        in_specs=(
            P("sp", None),
            P(("sp", "tp"), None),
            P(),
            P(),
            P(None, "tp"),
            P(),
            P(),
            P("sp", "tp"),
            P("sp", "tp"),
        ),
        out_specs=(P("sp", None), P(("sp", "tp"), None), P("sp", "tp")),
        check_vma=False,
    )
```

```python
import functools

import jax
import jax.numpy as jnp
from jax import lax
from jax.experimental import pallas as pl
from jax.experimental.pallas import tpu as pltpu
from jax.sharding import PartitionSpec as P

KVH = 2
HD = 128
EPS = 1e-06
GROUP = 4
CHUNKS = 4
MESH = pl.DeviceIdType.MESH
F32 = jnp.float32
BF16 = jnp.bfloat16

NT_DIMS = (((1,), (1,)), ((), ()))


def dot_nn(a, b):
    return jnp.dot(a, b, preferred_element_type=F32)


def dot_nt(a, b):
    return lax.dot_general(a, b, NT_DIMS, preferred_element_type=F32)


def inverse_rms(x):
    return lax.rsqrt(jnp.mean(x * x, axis=-1, keepdims=True) + EPS)


def norm_back(x, gain, cotangent):
    inv = inverse_rms(x)
    gc = cotangent * gain
    inner = jnp.mean(x * gc, axis=-1, keepdims=True)
    return inv * gc - x * (inv * inv * inv * inner)


def kernel(
    sp_size,
    tp_size,
    target_h,
    source_h,
    tgain_h,
    sgain_h,
    wq_h,
    wk_h,
    wv_h,
    att_h,
    dout_h,
    dtarget,
    dsource,
    dwq,
    target,
    source,
    tgain,
    sgain,
    wq,
    wk,
    wv,
    att,
    kvown,
    kvg,
    qg,
    og,
    qt,
    ot,
    delta,
    ntt,
    nttg,
    eb,
    pb,
    cmax,
    mrun,
    lrun,
    stat,
    dks,
    dkg,
    dkown,
    dkm,
    dkz,
    dqacc,
    dqs,
    dqr,
    dqm,
    dqz,
    dqg,
    dqx,
    rets,
    ret,
    dws,
    dwg,
    tkv_s,
    tkv_r,
    lkv_s,
    lkv_r,
    in_s,
    in_r,
    nt_s,
    nt_r,
    st_s,
    st_r,
    dk_s,
    dk_r,
    dc_s,
    dc_r,
    dy_s,
    dy_r,
    ag_s,
    ag_r,
    rt_s,
    rt_r,
    dx_s,
    dx_r,
    dw_s,
    dw_r,
    dz_s,
    dz_r,
    wx_s,
    wx_r,
    wf_s,
    wf_r,
    ld_s,
):
    outer = sp_size // GROUP
    rows = target.shape[0]
    width = wq.shape[2]
    heads = width // HD
    own_rows = source.shape[0]
    block = own_rows * tp_size
    group_rows = GROUP * rows
    scaling = HD ** (-0.5)
    sp = lax.axis_index("sp")
    t = lax.axis_index("tp")
    z = sp // GROUP
    g = sp % GROUP
    per_kv = tp_size // KVH
    sides = outer // 2
    side = z // 2
    par = lax.rem(z, 2)
    zp = z + 1 - 2 * par
    parts = wq_parts(heads)
    part_heads = heads // parts
    part_width = width // parts
    chunk = wq.shape[1] // (2 * CHUNKS)

    def tp_peer(o):
        return lax.rem(t + o, tp_size)

    def z_peer(o):
        return lax.rem(z + o, outer)

    def to_tp(p):
        return {"sp": sp, "tp": p}

    def to_g(p):
        return {"sp": z * GROUP + p, "tp": t}

    def to_z(p):
        return {"sp": p * GROUP + g, "tp": t}

    def copy(src, dst, ssem, rsem, dev):
        return pltpu.make_async_remote_copy(
            src_ref=src, dst_ref=dst, send_sem=ssem, recv_sem=rsem, device_id=dev, device_id_type=MESH
        )

    odd = lax.rem(g, 2)
    ga = g + 1 - 2 * odd
    gb = lax.rem(g + 2, GROUP)
    gc = lax.rem(ga + 2, GROUP)
    near = (g, ga, gb, gc)

    loads = [
        pltpu.make_async_copy(src, dst, ld_s.at[n])
        for n, (src, dst) in enumerate(
            (
                (dout_h, og.at[0]),
                (source_h, source),
                (sgain_h, sgain),
                (wk_h, wk),
                (wv_h, wv),
                (target_h, target),
                (tgain_h, tgain),
                (wq_h, wq.at[t]),
                (att_h, att),
            )
        )
    ]
    for load in loads:
        load.start()

    barrier = pltpu.get_barrier_semaphore()
    for o in range(1, tp_size):
        pl.semaphore_signal(barrier, inc=1, device_id=to_tp(tp_peer(o)), device_id_type=MESH)
    for p in near[1:]:
        pl.semaphore_signal(barrier, inc=1, device_id=to_g(p), device_id_type=MESH)
    for p in near[1:]:
        pl.semaphore_signal(barrier, inc=1, device_id={"sp": zp * GROUP + p, "tp": t}, device_id_type=MESH)
    for o in range(1, outer):
        pl.semaphore_signal(barrier, inc=1, device_id=to_z(z_peer(o)), device_id_type=MESH)

    def group_copy(k, way, slot, there):
        ref = (og, qg, delta)[k]
        return copy(ref.at[slot], ref.at[there], in_s.at[k, way], in_r.at[k, there], to_g((ga, gb, ga)[way]))

    def send_own(k):
        group_copy(k, 1, 0, 2).start()
        group_copy(k, 0, 0, 1).start()

    def forward(k):
        group_copy(k, 1, 0, 2).wait_recv()
        group_copy(k, 2, 2, 3).start()

    loads[0].wait()
    pl.semaphore_wait(barrier, tp_size + 2 * GROUP + outer - 4)
    send_own(0)
    for n in range(1, 5):
        loads[n].wait()
    s32 = source[...].astype(F32)
    ns = (s32 * inverse_rms(s32) * sgain[...]).astype(BF16)
    keys = dot_nn(ns, wk[...]).astype(BF16)
    values = dot_nn(ns, wv[...]).astype(BF16)
    for c in range(KVH):
        kvown[c, :, 0:HD] = keys[:, c * HD : (c + 1) * HD]
        kvown[c, :, HD : 2 * HD] = values[:, c * HD : (c + 1) * HD]
    kvg[z, t] = kvown[t // per_kv]

    def tkv(p, slot):
        return copy(kvown.at[p // per_kv], kvg.at[z, slot], tkv_s.at[p], tkv_r.at[slot], to_tp(p))

    def lkv(p, zslot, tslot):
        return copy(
            kvg.at[z, tslot], kvg.at[zslot, tslot], lkv_s.at[p, tslot], lkv_r.at[zslot, tslot], to_z(p)
        )

    def each_z(act):
        for dist in range(1, outer):

            @pl.when(z + dist < outer)
            def _():
                act(z + dist)

            @pl.when(z >= dist)
            def _():
                act(z - dist)

    for o in range(1, tp_size):
        tkv(tp_peer(o), t).start()
    each_z(lambda p: lkv(p, z, t).start())

    for n in range(5, 9):
        loads[n].wait()
    t32 = target[...].astype(F32)
    nt32 = t32 * inverse_rms(t32) * tgain[...]
    qg[0] = dot_nn(nt32.astype(BF16), wq[t]).astype(BF16)
    send_own(1)

    def half(slot, side, i):
        return wq.at[slot, pl.ds((side * CHUNKS + i) * chunk, chunk)]

    def wx_copy(p, slot, i):
        ref = half(slot, odd, i)
        return copy(ref, ref, wx_s.at[p, i], wx_r.at[slot, i], to_tp(p))

    def wf_copy(slot, side, i):
        ref = half(slot, side, i)
        return copy(ref, ref, wf_s.at[slot, i], wf_r.at[slot, i], to_g(ga))

    prod = (og[0].astype(F32) * att[...].astype(F32)).T
    drows = [jnp.sum(prod[h * HD : (h + 1) * HD], axis=0, keepdims=True) for h in range(heads)]
    drows.append(jnp.zeros((8 - heads, rows), F32))
    delta[0] = jnp.concatenate(drows, axis=0).astype(BF16).astype(F32)
    send_own(2)
    for i in range(CHUNKS):
        for o in range(1, tp_size):
            wx_copy(tp_peer(o), t, i).start()

    def columns_copy(zr, r):
        layer = (z, zp)[zr]
        p = near[r]
        return copy(
            ntt.at[:, lax.rem(layer, 2), p],
            nttg.at[zr, r],
            nt_s.at[zr, r],
            nt_r.at[zr, r],
            {"sp": layer * GROUP + p, "tp": t},
        )

    others = [(zr, r) for zr in (0, 1) for r in range(GROUP) if zr + r > 0]

    ntt[...] = nt32.T.astype(BF16).reshape(ntt.shape)
    nttg[0, 0] = ntt[:, par, g]
    for o in range(1, tp_size):
        p = tp_peer(o)
        tkv(t, p).wait_recv()
        each_z(lambda pz: lkv(pz, z, p).start())
    forward(0)
    forward(1)
    forward(2)
    for zr, r in others:
        columns_copy(zr, r).start()
    for r in (1, 3):
        for k in range(3):
            group_copy(k, 0, 0, r).wait_recv()

    def columns(ref, h):
        return ref[:, :, h * HD : (h + 1) * HD].reshape(group_rows, HD)

    for h in range(heads):
        qt[:, h * group_rows : (h + 1) * group_rows] = columns(qg, h).astype(F32).T.astype(BF16)
        ot[:, h * group_rows : (h + 1) * group_rows] = columns(og, h).astype(F32).T.astype(BF16)
    mrun[...] = jnp.full(mrun.shape, -jnp.inf, F32)
    lrun[...] = jnp.zeros(lrun.shape, F32)
    dqacc[...] = jnp.zeros(dqacc.shape, F32)

    low = jnp.minimum(z, outer - 1 - z)

    def in_turn(o):
        pos = jnp.where(o <= low, low - o, o)
        return jnp.where(z == low, pos, outer - 1 - pos)

    def score(zc, kb, kbt, vb, h):
        cols = slice(h * group_rows, (h + 1) * group_rows)
        s = dot_nn(kb, qt[:, cols])
        m_old = mrun[h : h + 1, :]
        m = jnp.maximum(m_old, jnp.max(s, axis=0, keepdims=True))
        e = jnp.exp((s - m) * scaling)
        keep = jnp.exp((m_old - m) * scaling)
        lrun[h : h + 1, :] = lrun[h : h + 1, :] * keep + jnp.sum(e, axis=0, keepdims=True)
        mrun[h : h + 1, :] = m
        cmax[zc, h : h + 1, :] = m
        drow = jnp.concatenate([delta[r, h : h + 1, :] for r in range(GROUP)], axis=1)
        p = (e * (dot_nn(vb, ot[:, cols]) - drow)).astype(BF16)
        eb[zc, :, cols] = e.astype(BF16)
        pb[zc, :, cols] = p
        dqacc[h] = dqacc[h] * keep + dot_nn(kbt, p)

    def operands(zc):
        kb = kvg[zc, :, :, 0:HD].reshape(block, HD)
        vb = kvg[zc, :, :, HD : 2 * HD].reshape(block, HD)
        return kb, kb.astype(F32).T.astype(BF16), vb

    def first(o, _):
        zc = in_turn(o)

        @pl.when(o > 0)
        def _():
            for ts in range(tp_size):
                lkv(zc, zc, ts).wait_recv()

        kb, kbt, vb = operands(zc)
        for h in range(heads):
            score(zc, kb, kbt, vb, h)
        return 0

    lax.fori_loop(0, outer - 1, first, 0)
    last = in_turn(outer - 1)
    for ts in range(tp_size):
        lkv(last, last, ts).wait_recv()

    def dc_copy(k, n):
        return copy(dqs.at[k, (1, 3)[n]], dqr.at[k, n], dc_s.at[k, n], dc_r.at[k, n], to_g(ga))

    def stat_copy(r):
        return copy(stat.at[0], stat.at[r], st_s.at[r], st_r.at[r], to_g(near[r]))

    kb, kbt, vb = operands(last)
    for k in range(parts):
        for h in range(k * part_heads, (k + 1) * part_heads):
            score(last, kb, kbt, vb, h)
            norm = scaling / lrun[h : h + 1, :]
            hh = h - k * part_heads
            for r in range(GROUP):
                cut = slice(r * rows, (r + 1) * rows)
                dqs[k, r, hh * HD : (hh + 1) * HD] = (dqacc[h, :, cut] * norm[:, cut]).astype(BF16)
        dc_copy(k, 1).start()
        dc_copy(k, 0).start()
    stat[0, 0:heads, :] = mrun[0:heads, :] * scaling + jnp.log(lrun[0:heads, :])
    if heads < 8:
        stat[0, heads:8, :] = jnp.zeros((8 - heads, group_rows), F32)
    for r in (1, 3, 2):
        stat_copy(r).start()

    def total_of(r):
        full = stat[r]
        return [full[:, (j ^ r) * rows : ((j ^ r) + 1) * rows] for j in range(GROUP)]

    def dy_copy(k):
        return copy(dqm.at[k], dqz.at[k], dy_s.at[k], dy_r.at[k], to_g(gb))

    stat_copy(1).wait_recv()
    own_total = total_of(0)
    pair_total = total_of(1)
    top = jnp.maximum(own_total[2], pair_total[2])
    own_w = jnp.exp(own_total[2] - top)
    pair_w = jnp.exp(pair_total[2] - top)
    inv = 1.0 / (own_w + pair_w)
    own_w = own_w * inv
    pair_w = pair_w * inv
    for k in range(parts):
        dc_copy(k, 1).wait_recv()
        for hh in range(part_heads):
            h = k * part_heads + hh
            cut = slice(hh * HD, (hh + 1) * HD)
            dqm[k, cut] = (
                dqs[k, 2, cut].astype(F32) * own_w[h : h + 1] + dqr[k, 1, cut].astype(F32) * pair_w[h : h + 1]
            ).astype(BF16)
        dy_copy(k).start()

    for r in (2, 3):
        stat_copy(r).wait_recv()
    totals = [jnp.concatenate(total_of(r), axis=1) for r in range(GROUP)]
    top = jnp.maximum(jnp.maximum(totals[0], totals[1]), jnp.maximum(totals[2], totals[3]))
    log_total = top + jnp.log(sum(jnp.exp(v - top) for v in totals))

    def dk_copy(i):
        return copy(dks.at[i], dkg.at[i], dk_s.at[i], dk_r.at[i], to_z(zp))

    def side_peer(o):
        return lax.rem(side + o, sides)

    def dz_copy(p, slot):
        return copy(dkm.at[p], dkz.at[slot], dz_s.at[p], dz_r.at[slot], to_z(2 * p + par))

    def source_grad(zc):
        factor = jnp.concatenate(
            [jnp.exp(cmax[zc, h : h + 1, :] * scaling - log_total[h : h + 1, :]) for h in range(heads)], axis=1
        )
        qf = (qt[...].astype(F32) * (factor * scaling)).astype(BF16)
        of = (ot[...].astype(F32) * factor).astype(BF16)
        return dot_nt(pb[zc], qf), dot_nt(eb[zc], of)

    def second(o, _):
        i = side_peer(1 + o)
        dk, dv = source_grad(2 * i + 1 - par)
        dks[i, :, 0:HD] = dk.astype(BF16)
        dks[i, :, HD : 2 * HD] = dv.astype(BF16)

        @pl.when(o < sides - 1)
        def _():
            dk_copy(i).start()

        return 0

    def third(o, _):
        i = side_peer(1 + o)
        dk, dv = source_grad(2 * i + par)
        dkown[i, :, 0:HD] = dk
        dkown[i, :, HD : 2 * HD] = dv
        return 0

    lax.fori_loop(0, sides, second, 0)
    ways = (
        (to_g(ga), (0, 0), (0, 1)),
        (to_g(gb), (0, 0), (0, 2)),
        (to_z(zp), (0, 0), (1, 0)),
        (to_g(ga), (0, 2), (0, 3)),
        (to_g(gb), (1, 0), (1, 2)),
        (to_g(ga), (1, 0), (1, 1)),
        (to_g(ga), (1, 2), (1, 3)),
    )

    def ag_copy(k, way):
        dev, (zf, rf), (zt, rt) = ways[way]
        return copy(dqg.at[k, zf, rf], dqg.at[k, zt, rt], ag_s.at[k, way], ag_r.at[k, way], dev)

    def dx_copy(k, p, slot):
        return copy(dqg.at[k, 0, 0], dqx.at[k, slot], dx_s.at[k, p], dx_r.at[k, slot], to_tp(p))

    weights = [jnp.exp(v[:, 0:rows] - log_total[:, 0:rows]) for v in totals]
    far_w = weights[2] + weights[3]
    for k in range(parts):
        dc_copy(k, 0).wait_recv()
        dy_copy(k).wait_recv()
        sums = []
        for hh in range(part_heads):
            h = k * part_heads + hh
            cut = slice(hh * HD, (hh + 1) * HD)
            sums.append(
                dqs[k, 0, cut].astype(F32) * weights[0][h : h + 1]
                + dqr[k, 0, cut].astype(F32) * weights[1][h : h + 1]
                + dqz[k, cut].astype(F32) * far_w[h : h + 1]
            )
        dqg[k, 0, 0] = jnp.concatenate(sums, axis=0).T.astype(BF16)
        for way in (2, 1, 0):
            ag_copy(k, way).start()
        for o in range(1, tp_size):
            dx_copy(k, tp_peer(o), t).start()
    dk_copy(side).start()
    lax.fori_loop(0, sides, third, 0)

    def forward_wq(i):
        for o in range(1, tp_size):
            p = tp_peer(o)
            wx_copy(t, p, i).wait_recv()
            wf_copy(p, odd, i).start()

    for i in range(CHUNKS - 2):
        forward_wq(i)
    for k in range(parts):
        ag_copy(k, 2).wait_recv()
        ag_copy(k, 4).start()
        ag_copy(k, 5).start()
        ag_copy(k, 1).wait_recv()
        ag_copy(k, 3).start()
        if k == 0:
            for o in range(1, sides):
                i = side_peer(o)
                dk_copy(i).wait_recv()
                dkm[i] = (dkown[i] + dkg[i].astype(F32)).astype(BF16)
                dz_copy(i, side).start()

    def dw_copy(k, p, slot):
        return copy(dws.at[k, p], dwg.at[k, slot], dw_s.at[k, p], dw_r.at[k, slot], to_z(2 * p + par))

    depth = ntt.shape[3]
    for i in range(CHUNKS - 2, CHUNKS):
        forward_wq(i)
    for zr, r in others:
        columns_copy(zr, r).wait_recv()
    for k in range(parts):
        ag_copy(k, 4).wait_recv()
        ag_copy(k, 6).start()
    lhs = jnp.concatenate(
        [nttg[zr, r].reshape(sides * depth, rows) for zr in (0, 1) for r in range(GROUP)], axis=1
    )
    for k in range(parts):
        for way in (0, 3, 5, 6):
            ag_copy(k, way).wait_recv()
        term = dot_nn(lhs, dqg[k].reshape(2 * group_rows, part_width))
        dws[k] = term.astype(BF16).reshape(dws.shape[1:])
        for o in range(1, sides):
            dw_copy(k, side_peer(o), side).start()

    dk_copy(side).wait_recv()
    total = dkown[side] + dkg[side].astype(F32)
    for o in range(1, sides):
        p = side_peer(o)
        dz_copy(p, p).wait_recv()
        total = total + dkz[p].astype(F32)
    rets[...] = total.astype(BF16).reshape(rets.shape)

    def ret_copy(p, slot):
        return copy(rets.at[p], ret.at[slot], rt_s.at[p], rt_r.at[slot], to_tp(p))

    for o in range(1, tp_size):
        ret_copy(tp_peer(o), t).start()
    ret[t] = rets[t]

    for k in range(parts):
        dqx[k, t] = dqg[k, 0, 0]
        for o in range(1, tp_size):
            p = tp_peer(o)
            dx_copy(k, p, p).wait_recv()
    for o in range(1, tp_size):
        for i in range(CHUNKS):
            wf_copy(tp_peer(o), 1 - odd, i).wait_recv()
    dn = jnp.zeros((rows, wq.shape[1]), F32)
    for p in range(tp_size):
        full = jnp.concatenate([dqx[k, p] for k in range(parts)], axis=1)
        dn = dn + dot_nt(full, wq[p])
    dtarget[...] = norm_back(target[...].astype(F32), tgain[...], dn).astype(BF16)

    for o in range(1, tp_size):
        p = tp_peer(o)
        ret_copy(p, p).wait_recv()
    dns = jnp.zeros(source.shape, F32)
    for c in range(KVH):
        part = ret[c * per_kv].astype(F32)
        for k in range(1, per_kv):
            part = part + ret[c * per_kv + k].astype(F32)
        part = part.astype(BF16)
        dns = dns + dot_nt(part[:, 0:HD], wk[:, c * HD : (c + 1) * HD])
        dns = dns + dot_nt(part[:, HD : 2 * HD], wv[:, c * HD : (c + 1) * HD])
    dsource[...] = norm_back(source[...].astype(F32), sgain[...], dns)

    for k in range(parts):
        dw_total = dws[k, side].astype(F32)
        for o in range(1, sides):
            p = side_peer(o)
            dw_copy(k, p, p).wait_recv()
            dw_total = dw_total + dwg[k, p].astype(F32)
        dwq[:, k * part_width : (k + 1) * part_width] = dw_total

    for o in range(1, tp_size):
        p = tp_peer(o)
        tkv(p, t).wait_send()
        ret_copy(p, t).wait_send()
        for k in range(parts):
            dx_copy(k, p, t).wait_send()
        for i in range(CHUNKS):
            wx_copy(p, t, i).wait_send()
            wf_copy(p, odd, i).wait_send()
    for k in range(3):
        group_copy(k, 0, 0, 1).wait_send()
        group_copy(k, 1, 0, 2).wait_send()
        group_copy(k, 2, 2, 3).wait_send()
    for zr, r in others:
        columns_copy(zr, r).wait_send()
    for r in (1, 2, 3):
        stat_copy(r).wait_send()
    for k in range(parts):
        dc_copy(k, 0).wait_send()
        dc_copy(k, 1).wait_send()
        dy_copy(k).wait_send()
        for way in range(7):
            ag_copy(k, way).wait_send()
    for o in range(1, outer):
        p = z_peer(o)
        for ts in range(tp_size):
            lkv(p, z, ts).wait_send()
    dk_copy(side).wait_send()
    for o in range(1, sides):
        p = side_peer(o)
        dk_copy(p).wait_send()
        dz_copy(p, side).wait_send()
        for k in range(parts):
            dw_copy(k, p, side).wait_send()


def wq_parts(heads):
    return 2 if heads % 2 == 0 else 1


def local(target, source, target_gain, source_gain, w_query, w_key, w_value, attended, d_attended):
    sp_size = lax.axis_size("sp")
    tp_size = lax.axis_size("tp")
    outer = sp_size // GROUP
    sides = outer // 2
    rows, d = target.shape
    own_rows = source.shape[0]
    block = own_rows * tp_size
    width = w_query.shape[1]
    heads = width // HD
    depth = d // sp_size
    group_rows = GROUP * rows
    vmem = pltpu.VMEM
    dma = pltpu.SemaphoreType.DMA
    parts = wq_parts(heads)
    part_width = width // parts
    scratch = [
        vmem((rows, d), BF16),
        vmem((own_rows, d), BF16),
        vmem((1, d), F32),
        vmem((1, d), F32),
        vmem((tp_size, d, width), BF16),
        vmem(w_key.shape, BF16),
        vmem(w_value.shape, BF16),
        vmem((rows, width), BF16),
        vmem((KVH, own_rows, 2 * HD), BF16),
        vmem((outer, tp_size, own_rows, 2 * HD), BF16),
        vmem((GROUP, rows, width), BF16),
        vmem((GROUP, rows, width), BF16),
        vmem((HD, heads * group_rows), BF16),
        vmem((HD, heads * group_rows), BF16),
        vmem((GROUP, 8, rows), F32),
        vmem((sides, 2, GROUP, depth, rows), BF16),
        vmem((2, GROUP, sides, depth, rows), BF16),
        vmem((outer, block, heads * group_rows), BF16),
        vmem((outer, block, heads * group_rows), BF16),
        vmem((outer, 8, group_rows), F32),
        vmem((8, group_rows), F32),
        vmem((8, group_rows), F32),
        vmem((GROUP, 8, group_rows), F32),
        vmem((sides, block, 2 * HD), BF16),
        vmem((sides, block, 2 * HD), BF16),
        vmem((sides, block, 2 * HD), F32),
        vmem((sides, block, 2 * HD), BF16),
        vmem((sides, block, 2 * HD), BF16),
        vmem((heads, HD, group_rows), F32),
        vmem((parts, GROUP, part_width, rows), BF16),
        vmem((parts, 2, part_width, rows), BF16),
        vmem((parts, part_width, rows), BF16),
        vmem((parts, part_width, rows), BF16),
        vmem((parts, 2, GROUP, rows, part_width), BF16),
        vmem((parts, tp_size, rows, part_width), BF16),
        vmem((tp_size, own_rows, 2 * HD), BF16),
        vmem((tp_size, own_rows, 2 * HD), BF16),
        vmem((parts, sides, depth, part_width), BF16),
        vmem((parts, sides, depth, part_width), BF16),
    ]
    sems = [
        dma((tp_size,)),
        dma((tp_size,)),
        dma((outer, tp_size)),
        dma((outer, tp_size)),
        dma((3, 3)),
        dma((3, GROUP)),
        dma((2, GROUP)),
        dma((2, GROUP)),
        dma((GROUP,)),
        dma((GROUP,)),
        dma((sides,)),
        dma((sides,)),
        dma((parts, 2)),
        dma((parts, 2)),
        dma((parts,)),
        dma((parts,)),
        dma((parts, 7)),
        dma((parts, 7)),
        dma((tp_size,)),
        dma((tp_size,)),
        dma((parts, tp_size)),
        dma((parts, tp_size)),
        dma((parts, sides)),
        dma((parts, sides)),
        dma((sides,)),
        dma((sides,)),
        dma((tp_size, CHUNKS)),
        dma((tp_size, CHUNKS)),
        dma((tp_size, CHUNKS)),
        dma((tp_size, CHUNKS)),
        dma((9,)),
    ]
    spec = pl.BlockSpec(memory_space=pl.ANY)
    held = pl.pallas_call(
        functools.partial(kernel, sp_size, tp_size),
        out_shape=(
            pltpu.VMEM((rows, d), BF16),
            pltpu.VMEM((own_rows, d), F32),
            pltpu.VMEM((depth, width), F32),
        ),
        in_specs=[spec] * 9,
        out_specs=(pl.BlockSpec(memory_space=pltpu.VMEM),) * 3,
        scratch_shapes=scratch + sems,
        compiler_params=pltpu.CompilerParams(
            collective_id=0, has_side_effects=True, vmem_limit_bytes=60000 * 1024
        ),
    )(
        *[
            pltpu.with_memory_space_constraint(x, pltpu.HBM)
            for x in (
                target,
                source,
                target_gain.reshape(1, d),
                source_gain.reshape(1, d),
                w_query,
                w_key,
                w_value,
                attended,
                d_attended,
            )
        ]
    )

    return pl.pallas_call(
        store_kernel,
        out_shape=(
            jax.ShapeDtypeStruct((rows, d), BF16),
            jax.ShapeDtypeStruct((own_rows, d), F32),
            jax.ShapeDtypeStruct((depth, width), F32),
        ),
        in_specs=[pl.BlockSpec(memory_space=pltpu.VMEM)] * 3,
        out_specs=(spec,) * 3,
        scratch_shapes=[dma((3,))],
    )(*[pltpu.with_memory_space_constraint(x, pltpu.VMEM) for x in held])


def store_kernel(a, b, c, a_h, b_h, c_h, sem):
    stores = [
        pltpu.make_async_copy(src, dst, sem.at[n])
        for n, (src, dst) in enumerate(((a, a_h), (b, b_h), (c, c_h)))
    ]
    for store in stores:
        store.start()
    for store in stores:
        store.wait()


def solution(mesh):
    return jax.shard_map(
        local,
        mesh=mesh,
        in_specs=(
            P("sp", None),
            P(("sp", "tp"), None),
            P(),
            P(),
            P(None, "tp"),
            P(),
            P(),
            P("sp", "tp"),
            P("sp", "tp"),
        ),
        out_specs=(P("sp", None), P(("sp", "tp"), None), P("sp", "tp")),
        check_vma=False,
    )
```

```python
import functools

import jax
import jax.numpy as jnp
from jax import lax
from jax.experimental import pallas as pl
from jax.experimental.pallas import tpu as pltpu
from jax.sharding import PartitionSpec as P

KVH = 2
HD = 128
EPS = 1e-06
GROUP = 4
CHUNKS = 4
LOG2E = 1.4426950408889634
MESH = pl.DeviceIdType.MESH
F32 = jnp.float32
BF16 = jnp.bfloat16

NT_DIMS = (((1,), (1,)), ((), ()))


def dot_nn(a, b):
    return jnp.dot(a, b, preferred_element_type=F32)


def dot_nt(a, b):
    return lax.dot_general(a, b, NT_DIMS, preferred_element_type=F32)


def inverse_rms(x):
    return lax.rsqrt(jnp.mean(x * x, axis=-1, keepdims=True) + EPS)


def norm_back(x, gain, cotangent):
    inv = inverse_rms(x)
    gc = cotangent * gain
    inner = jnp.mean(x * gc, axis=-1, keepdims=True)
    return inv * gc - x * (inv * inv * inv * inner)


def kernel(
    sp_size,
    tp_size,
    target_h,
    source_h,
    tgain_h,
    sgain_h,
    wq_h,
    wk_h,
    wv_h,
    att_h,
    dout_h,
    dtarget,
    dsource,
    dwq,
    target,
    source,
    tgain,
    sgain,
    wq,
    wk,
    wv,
    att,
    kvown,
    kvg,
    ktg,
    qg,
    og,
    qt,
    ot,
    delta,
    ntt,
    nttg,
    eb,
    pb,
    cmax,
    mrun,
    lrun,
    stat,
    psend,
    pget,
    dks,
    dkg,
    dkown,
    dkm,
    dkz,
    dqacc,
    dqs,
    dqr,
    dqm,
    dqz,
    dqg,
    dqx,
    rets,
    ret,
    dws,
    dwg,
    tkv_s,
    tkv_r,
    lkv_s,
    lkv_r,
    rl_s,
    in_s,
    in_r,
    nt_s,
    nt_r,
    st_s,
    st_r,
    ps_s,
    ps_r,
    dk_s,
    dk_r,
    dc_s,
    dc_r,
    dy_s,
    dy_r,
    ag_s,
    ag_r,
    rt_s,
    rt_r,
    dx_s,
    dx_r,
    dw_s,
    dw_r,
    dz_s,
    dz_r,
    wx_s,
    wx_r,
    wf_s,
    wf_r,
    ld_s,
):
    outer = sp_size // GROUP
    rows = target.shape[0]
    width = wq.shape[2]
    heads = width // HD
    own_rows = source.shape[0]
    block = own_rows * tp_size
    group_rows = GROUP * rows
    scaling = HD ** (-0.5)
    sp = lax.axis_index("sp")
    t = lax.axis_index("tp")
    z = sp // GROUP
    g = sp % GROUP
    per_kv = tp_size // KVH
    sides = outer // 2
    side = z // 2
    par = lax.rem(z, 2)
    zp = z + 1 - 2 * par
    parts = wq_parts(heads)
    part_heads = heads // parts
    part_width = width // parts
    chunk = wq.shape[1] // (2 * CHUNKS)

    def tp_peer(o):
        return lax.rem(t + o, tp_size)

    def z_peer(o):
        return lax.rem(z + o, outer)

    def to_tp(p):
        return {"sp": sp, "tp": p}

    def to_g(p):
        return {"sp": z * GROUP + p, "tp": t}

    def to_z(p):
        return {"sp": p * GROUP + g, "tp": t}

    def copy(src, dst, ssem, rsem, dev):
        return pltpu.make_async_remote_copy(
            src_ref=src, dst_ref=dst, send_sem=ssem, recv_sem=rsem, device_id=dev, device_id_type=MESH
        )

    def all_sent(ref, sem):
        copy(ref, ref, sem, sem, to_g(ga)).wait_send()

    def all_here(ref, sem):
        copy(ref, ref, sem, sem, to_g(ga)).wait_recv()

    odd = lax.rem(g, 2)
    ga = g + 1 - 2 * odd
    gb = lax.rem(g + 2, GROUP)
    gc = lax.rem(ga + 2, GROUP)
    near = (g, ga, gb, gc)

    loads = [
        pltpu.make_async_copy(src, dst, ld_s.at[n])
        for n, (src, dst) in enumerate(
            (
                (dout_h, og.at[0]),
                (source_h, source),
                (sgain_h, sgain),
                (wk_h, wk),
                (wv_h, wv),
                (target_h, target),
                (tgain_h, tgain),
                (wq_h, wq.at[t]),
                (att_h, att),
            )
        )
    ]
    for load in loads:
        load.start()

    barrier = pltpu.get_barrier_semaphore()
    for o in range(1, tp_size):
        pl.semaphore_signal(barrier, inc=1, device_id=to_tp(tp_peer(o)), device_id_type=MESH)
    for p in near[1:]:
        pl.semaphore_signal(barrier, inc=1, device_id=to_g(p), device_id_type=MESH)
    for p in near[1:]:
        pl.semaphore_signal(barrier, inc=1, device_id={"sp": zp * GROUP + p, "tp": t}, device_id_type=MESH)
    for o in range(1, outer):
        pl.semaphore_signal(barrier, inc=1, device_id=to_z(z_peer(o)), device_id_type=MESH)

    def group_copy(k, way, slot, there):
        ref = (og, qg, delta)[k]
        shared = max(k, 1) if there != 2 else k
        return copy(
            ref.at[slot], ref.at[there], in_s.at[k], in_r.at[shared, there], to_g((ga, gb, ga)[way])
        )

    def group_here(r):
        all_here(og.at[0:2], in_r.at[1, r])
        all_here(delta.at[0], in_r.at[2, r])

    def send_own(k):
        group_copy(k, 1, 0, 2).start()
        group_copy(k, 0, 0, 1).start()

    def forward(k):
        group_copy(k, 1, 0, 2).wait_recv()
        group_copy(k, 2, 2, 3).start()

    loads[0].wait()
    pl.semaphore_wait(barrier, tp_size + 2 * GROUP + outer - 4)
    send_own(0)
    for n in range(1, 5):
        loads[n].wait()
    s32 = source[...].astype(F32)
    ns = (s32 * inverse_rms(s32) * sgain[...]).astype(BF16)
    keys = dot_nn(ns, wk[...]).astype(BF16)
    values = dot_nn(ns, wv[...]).astype(BF16)
    for c in range(KVH):
        kvown[c, :, 0:HD] = keys[:, c * HD : (c + 1) * HD]
        kvown[c, :, HD : 2 * HD] = values[:, c * HD : (c + 1) * HD]
    kvg[z, t] = kvown[t // per_kv]

    def tkv(p, slot):
        return copy(kvown.at[p // per_kv], kvg.at[z, slot], tkv_s, tkv_r.at[slot], to_tp(p))

    def lkv(p, zslot, tslot):
        return copy(
            kvg.at[z, tslot], kvg.at[zslot, tslot], lkv_s, lkv_r.at[zslot, tslot], to_z(p)
        )

    def relay(zslot, tslot):
        ref = kvg.at[zslot, tslot]
        return copy(ref, ref, rl_s.at[zslot], lkv_r.at[zslot, tslot], to_z(zp))

    def each_rep(act):
        act(zp)
        for o in range(1, sides):
            p = lax.rem(side + o, sides)
            act(jnp.where(p > side, 2 * p, 2 * p + 1))

    def each_relay(dist, act):
        @pl.when((par == 0) & (z >= dist))
        def _():
            act(z - dist)

        @pl.when((par == 1) & (z + dist < outer))
        def _():
            act(z + dist)

    def pass_on(dist, ts):
        def act(p):
            lkv(p, p, ts).wait_recv()
            relay(p, ts).start()

        each_relay(dist, act)

    for o in range(1, tp_size):
        tkv(tp_peer(o), t).start()
    each_rep(lambda p: lkv(p, z, t).start())

    for n in range(5, 9):
        loads[n].wait()
    t32 = target[...].astype(F32)
    nt32 = t32 * inverse_rms(t32) * tgain[...]
    qg[0] = dot_nn(nt32.astype(BF16), wq[t]).astype(BF16)
    send_own(1)

    def half(slot, side, i):
        return wq.at[slot, pl.ds((side * CHUNKS + i) * chunk, chunk)]

    def wx_copy(p, slot, i):
        ref = half(slot, odd, i)
        return copy(ref, ref, wx_s, wx_r.at[i], to_tp(p))

    def wf_copy(slot, side, i):
        ref = half(slot, side, i)
        return copy(ref, ref, wf_s, wf_r, to_g(ga))

    prod = (og[0].astype(F32) * att[...].astype(F32)).T
    drows = [jnp.sum(prod[h * HD : (h + 1) * HD], axis=0, keepdims=True) for h in range(heads)]
    drows.append(jnp.zeros((8 - heads, rows), F32))
    delta[0] = jnp.concatenate(drows, axis=0).astype(BF16).astype(F32)
    send_own(2)

    def columns_copy(zr, r):
        layer = (z, zp)[zr]
        p = near[r]
        return copy(
            ntt.at[:, lax.rem(layer, 2), p],
            nttg.at[zr * GROUP + r],
            nt_s,
            nt_r,
            {"sp": layer * GROUP + p, "tp": t},
        )

    ntt[...] = nt32.T.astype(BF16).reshape(ntt.shape)
    nttg[0] = ntt[:, par, g]
    for o in range(1, tp_size):
        p = tp_peer(o)
        tkv(t, p).wait_recv()
        each_rep(lambda pz: lkv(pz, z, p).start())
    for i in range(CHUNKS):
        for o in range(1, tp_size):
            wx_copy(tp_peer(o), t, i).start()
    group_here(1)

    def turned(blocks):
        for r in blocks:
            for h in range(heads):
                cut = slice(h * group_rows + r * rows, h * group_rows + (r + 1) * rows)
                qt[:, cut] = qg[r, :, h * HD : (h + 1) * HD].astype(F32).T.astype(BF16)
                ot[:, cut] = og[r, :, h * HD : (h + 1) * HD].astype(F32).T.astype(BF16)

    turned((0, 1))
    mrun[...] = jnp.full(mrun.shape, -jnp.inf, F32)
    lrun[...] = jnp.zeros(lrun.shape, F32)
    dqacc[...] = jnp.zeros(dqacc.shape, F32)

    low = jnp.minimum(z, outer - 1 - z)

    def in_turn(o):
        pos = jnp.where(o <= low, low - o, o)
        return jnp.where(z == low, pos, outer - 1 - pos)

    def key_turn(zc):
        ktg[zc] = kvg[zc, :, :, 0:HD].reshape(block, HD).astype(F32).T.astype(BF16)

    half_rows = group_rows // 2
    steep = scaling * LOG2E

    def score(zc, tiles, done=None):
        kb = kvg[zc, :, :, 0:HD].reshape(block, HD)
        vb = kvg[zc, :, :, HD : 2 * HD].reshape(block, HD)
        kbt = ktg[zc]

        def products(h, side_of):
            cut = slice(h * group_rows + side_of * half_rows, h * group_rows + (side_of + 1) * half_rows)
            return dot_nn(kb, qt[:, cut]), dot_nn(vb, ot[:, cut])

        def gather(h, side_of, cut, keep, p):
            dqacc[h, :, cut] = dqacc[h, :, cut] * keep + dot_nn(kbt, p)
            if done is not None and side_of == 1:
                done(h)

        ready = products(*tiles[0])
        held = None
        for n, (h, side_of) in enumerate(tiles):
            s, dw = ready
            if n + 1 < len(tiles):
                ready = products(*tiles[n + 1])
            cut = slice(side_of * half_rows, (side_of + 1) * half_rows)
            wide = slice(h * group_rows + side_of * half_rows, h * group_rows + (side_of + 1) * half_rows)
            m_old = mrun[h : h + 1, cut]
            m = jnp.maximum(m_old, jnp.max(s, axis=0, keepdims=True))
            e = jnp.exp2(s * steep - m * steep)
            keep = jnp.exp2((m_old - m) * steep)
            lrun[h : h + 1, cut] = lrun[h : h + 1, cut] * keep + jnp.sum(e, axis=0, keepdims=True)
            mrun[h : h + 1, cut] = m
            cmax[zc, h : h + 1, cut] = m
            drow = jnp.concatenate([delta[2 * side_of + i, h : h + 1, :] for i in range(2)], axis=1)
            short = e.astype(BF16)
            p = short * (dw - drow).astype(BF16)
            eb[zc, :, wide] = short
            pb[zc, :, wide] = p
            if held is not None:
                gather(*held)
            held = (h, side_of, cut, keep, p)
        gather(*held)

    def arrive(zc):
        for ts in range(tp_size):
            lkv(zc, zc, ts).wait_recv()

    def waits(zc):
        relayed = ((par == 0) & (zc < z)) | ((par == 1) & (zc > z))

        @pl.when(jnp.logical_not(relayed))
        def _():
            arrive(zc)

    near_tiles = [(h, 0) for h in range(heads)]
    far_tiles = [(h, 1) for h in range(heads)]
    later = [tp_peer(o) for o in range(1, tp_size)]

    pass_on(1, t)
    key_turn(z)
    score(z, near_tiles)
    forward(0)
    pass_on(2, t)
    for p in later:
        pass_on(1, p)
    one = in_turn(1)
    waits(one)
    key_turn(one)
    score(one, near_tiles)
    forward(1)
    forward(2)
    for p in later:
        pass_on(2, p)
    for dist in range(3, outer):
        for ts in range(tp_size):
            pass_on(dist, ts)
    for r in (3, 2, 1):
        columns_copy(0, r).start()
    for r in (3, 2, 0, 1):
        columns_copy(1, r).start()
    group_here(3)
    turned((2, 3))

    def far(o, _):
        score(in_turn(o), far_tiles)
        return 0

    def first(o, _):
        zc = in_turn(o)
        waits(zc)
        key_turn(zc)
        score(zc, near_tiles + far_tiles)
        return 0

    lax.fori_loop(0, 2, far, 0)
    lax.fori_loop(2, outer - 1, first, 0)
    last = in_turn(outer - 1)
    waits(last)
    key_turn(last)

    def dc_copy(k, n):
        return copy(dqs.at[k, (1, 3)[n]], dqr.at[n, k], dc_s, dc_r.at[k * n + n], to_g(ga))

    def ps_copy(k):
        return copy(psend.at[k], pget.at[k], ps_s, ps_r.at[k], to_g(ga))

    def stat_copy(r):
        return copy(stat.at[0], stat.at[r], st_s, st_r, to_g(near[r]))

    def release(h):
        k = h // part_heads
        hh = h % part_heads
        norm = scaling / lrun[h : h + 1, :]
        for r in range(GROUP):
            cut = slice(r * rows, (r + 1) * rows)
            dqs[k, r, hh * HD : (hh + 1) * HD] = (dqacc[h, :, cut] * norm[:, cut]).astype(BF16)
        if hh == part_heads - 1:
            part = range(k * part_heads, (k + 1) * part_heads)
            logs = [mrun[j : j + 1, :] * scaling + jnp.log(lrun[j : j + 1, :]) for j in part]
            psend[k] = jnp.concatenate(logs + [jnp.zeros((8 - part_heads, group_rows), F32)], axis=0)
            ps_copy(k).start()
            dc_copy(k, 1).start()
            dc_copy(k, 0).start()

    score(last, [(h, side_of) for h in range(heads) for side_of in (0, 1)], release)
    stat[0] = jnp.concatenate(
        [psend[k, 0:part_heads] for k in range(parts)] + [jnp.zeros((8 - heads, group_rows), F32)], axis=0
    )
    for r in (3, 2, 1):
        stat_copy(r).start()

    def in_order(full, r):
        return [full[:, (j ^ r) * rows : ((j ^ r) + 1) * rows] for j in range(GROUP)]

    def dy_copy(k):
        return copy(dqm.at[k], dqz.at[k], dy_s, dy_r.at[k], to_g(gb))

    for k in range(parts):
        ps_copy(k).wait_recv()
        dc_copy(k, 1).wait_recv()
        mine = in_order(psend[k], 0)[2]
        pairs = in_order(pget[k], 1)[2]
        top = jnp.maximum(mine, pairs)
        own_w = jnp.exp(mine - top)
        pair_w = jnp.exp(pairs - top)
        inv = 1.0 / (own_w + pair_w)
        own_w = own_w * inv
        pair_w = pair_w * inv
        for hh in range(part_heads):
            cut = slice(hh * HD, (hh + 1) * HD)
            dqm[k, cut] = (
                dqs[k, 2, cut].astype(F32) * own_w[hh : hh + 1] + dqr[1, k, cut].astype(F32) * pair_w[hh : hh + 1]
            ).astype(BF16)
        dy_copy(k).start()

    all_here(stat.at[1:GROUP], st_r)
    totals = [jnp.concatenate(in_order(stat[r], r), axis=1) for r in range(GROUP)]
    top = jnp.maximum(jnp.maximum(totals[0], totals[1]), jnp.maximum(totals[2], totals[3]))
    log_total = top + jnp.log(sum(jnp.exp(v - top) for v in totals))

    def dk_copy(i, n):
        return copy(dks.at[i, n], dkg.at[i, n], dk_s, dk_r.at[i, n], to_z(zp))

    def side_peer(o):
        return lax.rem(side + o, sides)

    def dz_copy(p, slot, n):
        return copy(dkm.at[p, n], dkz.at[slot, n], dz_s, dz_r, to_z(2 * p + par))

    def source_grad(zc, put):
        factor = jnp.concatenate(
            [jnp.exp(cmax[zc, h : h + 1, :] * scaling - log_total[h : h + 1, :]) for h in range(heads)], axis=1
        )
        qf = (qt[...].astype(F32) * (factor * scaling)).astype(BF16)
        put(0, dot_nt(pb[zc], qf))
        of = (ot[...].astype(F32) * factor).astype(BF16)
        put(1, dot_nt(eb[zc], of))

    def other(i, send):
        def put(n, value):
            dks[i, n] = value.astype(BF16)
            if send:
                dk_copy(i, n).start()

        source_grad(2 * i + 1 - par, put)

    def mine(i):
        def put(n, value):
            dkown[i, n] = value

        source_grad(2 * i + par, put)

    for o in range(1, sides):
        other(side_peer(o), True)
    for o in range(1, sides):
        mine(side_peer(o))

    ways = (
        (to_g(ga), (0, 0), (0, 1)),
        (to_g(gb), (0, 0), (0, 2)),
        (to_z(zp), (0, 0), (1, 0)),
        (to_g(ga), (0, 2), (0, 3)),
        (to_g(gb), (1, 0), (1, 2)),
        (to_g(ga), (1, 0), (1, 1)),
        (to_g(ga), (1, 2), (1, 3)),
    )

    def ag_copy(k, way):
        dev, (zf, rf), (zt, rt) = ways[way]
        arrival = {1: 0, 2: 1, 4: 2}.get(way, 3)
        return copy(dqg.at[k, zf, rf], dqg.at[k, zt, rt], ag_s.at[way // 4], ag_r.at[k, arrival], dev)

    def dx_copy(k, p, slot):
        return copy(dqg.at[k, 0, 0], dqx.at[k, slot], dx_s, dx_r, to_tp(p))

    all_here(dqr.at[0], dc_r.at[0])
    weights = [jnp.exp(v[:, 0:rows] - log_total[:, 0:rows]) for v in totals]
    far_w = weights[2] + weights[3]
    for k in range(parts):
        dy_copy(k).wait_recv()
        sums = []
        for hh in range(part_heads):
            h = k * part_heads + hh
            cut = slice(hh * HD, (hh + 1) * HD)
            sums.append(
                dqs[k, 0, cut].astype(F32) * weights[0][h : h + 1]
                + dqr[0, k, cut].astype(F32) * weights[1][h : h + 1]
                + dqz[k, cut].astype(F32) * far_w[h : h + 1]
            )
        dqg[k, 0, 0] = jnp.concatenate(sums, axis=0).T.astype(BF16)
        for way in (2, 1, 0):
            ag_copy(k, way).start()
        for o in range(1, tp_size):
            dx_copy(k, tp_peer(o), t).start()
    other(side, False)
    mine(side)

    def forward_wq(i):
        all_here(wq.at[0 : tp_size - 1, 0:chunk], wx_r.at[i])
        for o in range(1, tp_size):
            wf_copy(tp_peer(o), odd, i).start()

    for i in range(CHUNKS - 2):
        forward_wq(i)
    for o in range(1, sides):
        i = side_peer(o)
        for n in range(2):
            dk_copy(i, n).wait_recv()
            dkm[i, n] = (dkown[i, n] + dkg[i, n].astype(F32)).astype(BF16)
            dz_copy(i, side, n).start()
    for n in range(2):
        dk_copy(side, n).start()
    for k in range(parts):
        ag_copy(k, 2).wait_recv()
        ag_copy(k, 4).start()
        ag_copy(k, 5).start()
        ag_copy(k, 1).wait_recv()
        ag_copy(k, 3).start()

    def dw_copy(k, p, slot):
        return copy(dws.at[k, p], dwg.at[k, slot], dw_s, dw_r.at[k], to_z(2 * p + par))

    depth = ntt.shape[3]
    for i in range(CHUNKS - 2, CHUNKS):
        forward_wq(i)
    all_here(nttg.at[1 : 2 * GROUP], nt_r)
    lhs = jnp.concatenate(
        [nttg[n].reshape(sides * depth, rows) for n in range(2 * GROUP)], axis=1
    )

    def weight_grad(k):
        all_here(dqg.at[k, 0], ag_r.at[k, 3])
        term = dot_nn(lhs, dqg[k].reshape(2 * group_rows, part_width))
        dws[k] = term.astype(BF16).reshape(dws.shape[1:])
        for o in range(1, sides):
            dw_copy(k, side_peer(o), side).start()

    for k in range(parts):
        ag_copy(k, 4).wait_recv()
        ag_copy(k, 6).start()
        if k > 0:
            weight_grad(k - 1)
    weight_grad(parts - 1)

    all_here(dkz.at[0 : sides - 1], dz_r)
    totals_kv = []
    for n in range(2):
        dk_copy(side, n).wait_recv()
        total = dkown[side, n] + dkg[side, n].astype(F32)
        for o in range(1, sides):
            p = side_peer(o)
            total = total + dkz[p, n].astype(F32)
        totals_kv.append(total)
    rets[...] = jnp.concatenate(totals_kv, axis=1).astype(BF16).reshape(rets.shape)

    def ret_copy(p, slot):
        return copy(rets.at[p], ret.at[slot], rt_s, rt_r, to_tp(p))

    for o in range(1, tp_size):
        ret_copy(tp_peer(o), t).start()
    ret[t] = rets[t]

    for k in range(parts):
        dqx[k, t] = dqg[k, 0, 0]
    all_here(dqx.at[:, 0 : tp_size - 1], dx_r)
    all_here(wq.at[0 : tp_size - 1, 0 : CHUNKS * chunk], wf_r)
    dn = jnp.zeros((rows, wq.shape[1]), F32)
    for p in range(tp_size):
        full = jnp.concatenate([dqx[k, p] for k in range(parts)], axis=1)
        dn = dn + dot_nt(full, wq[p])
    dtarget[...] = norm_back(target[...].astype(F32), tgain[...], dn).astype(BF16)

    all_here(ret.at[0 : tp_size - 1], rt_r)
    dns = jnp.zeros(source.shape, F32)
    for c in range(KVH):
        part = ret[c * per_kv].astype(F32)
        for k in range(1, per_kv):
            part = part + ret[c * per_kv + k].astype(F32)
        part = part.astype(BF16)
        dns = dns + dot_nt(part[:, 0:HD], wk[:, c * HD : (c + 1) * HD])
        dns = dns + dot_nt(part[:, HD : 2 * HD], wv[:, c * HD : (c + 1) * HD])
    dsource[...] = norm_back(source[...].astype(F32), sgain[...], dns)

    for k in range(parts):
        dw_total = dws[k, side].astype(F32)
        all_here(dwg.at[k, 0 : sides - 1], dw_r.at[k])
        for o in range(1, sides):
            p = side_peer(o)
            dw_total = dw_total + dwg[k, p].astype(F32)
        dwq[:, k * part_width : (k + 1) * part_width] = dw_total

    all_sent(kvg.at[0, 0 : tp_size - 1], tkv_s)
    all_sent(kvg.at[0:sides], lkv_s)
    for dist in range(1, outer):
        each_relay(dist, lambda p: all_sent(kvg.at[p], rl_s.at[p]))
    all_sent(rets.at[0 : tp_size - 1], rt_s)
    all_sent(dqx.at[:, 0 : tp_size - 1], dx_s)
    all_sent(wq.at[0 : tp_size - 1, 0 : CHUNKS * chunk], wx_s)
    all_sent(wq.at[0 : tp_size - 1, 0 : CHUNKS * chunk], wf_s)
    for k, ref in enumerate((og, qg, delta)):
        all_sent(ref.at[0:3], in_s.at[k])
    all_sent(nttg.at[1 : 2 * GROUP], nt_s)
    all_sent(stat.at[1:GROUP], st_s)
    all_sent(psend, ps_s)
    all_sent(dqr, dc_s)
    all_sent(dqm, dy_s)
    all_sent(dqg.at[:, 0], ag_s.at[0])
    all_sent(dqg.at[:, 0, 0:3], ag_s.at[1])
    all_sent(dks, dk_s)
    all_sent(dkm.at[0 : sides - 1], dz_s)
    all_sent(dws.at[:, 0 : sides - 1], dw_s)


def wq_parts(heads):
    return heads


def local(target, source, target_gain, source_gain, w_query, w_key, w_value, attended, d_attended):
    sp_size = lax.axis_size("sp")
    tp_size = lax.axis_size("tp")
    outer = sp_size // GROUP
    sides = outer // 2
    rows, d = target.shape
    own_rows = source.shape[0]
    block = own_rows * tp_size
    width = w_query.shape[1]
    heads = width // HD
    depth = d // sp_size
    group_rows = GROUP * rows
    vmem = pltpu.VMEM
    dma = pltpu.SemaphoreType.DMA
    parts = wq_parts(heads)
    part_width = width // parts
    scratch = [
        vmem((rows, d), BF16),
        vmem((own_rows, d), BF16),
        vmem((1, d), F32),
        vmem((1, d), F32),
        vmem((tp_size, d, width), BF16),
        vmem(w_key.shape, BF16),
        vmem(w_value.shape, BF16),
        vmem((rows, width), BF16),
        vmem((KVH, own_rows, 2 * HD), BF16),
        vmem((outer, tp_size, own_rows, 2 * HD), BF16),
        vmem((outer, HD, block), BF16),
        vmem((GROUP, rows, width), BF16),
        vmem((GROUP, rows, width), BF16),
        vmem((HD, heads * group_rows), BF16),
        vmem((HD, heads * group_rows), BF16),
        vmem((GROUP, 8, rows), F32),
        vmem((sides, 2, GROUP, depth, rows), BF16),
        vmem((2 * GROUP, sides, depth, rows), BF16),
        vmem((outer, block, heads * group_rows), BF16),
        vmem((outer, block, heads * group_rows), BF16),
        vmem((outer, 8, group_rows), F32),
        vmem((8, group_rows), F32),
        vmem((8, group_rows), F32),
        vmem((GROUP, 8, group_rows), F32),
        vmem((parts, 8, group_rows), F32),
        vmem((parts, 8, group_rows), F32),
        vmem((sides, 2, block, HD), BF16),
        vmem((sides, 2, block, HD), BF16),
        vmem((sides, 2, block, HD), F32),
        vmem((sides, 2, block, HD), BF16),
        vmem((sides, 2, block, HD), BF16),
        vmem((heads, HD, group_rows), F32),
        vmem((parts, GROUP, part_width, rows), BF16),
        vmem((2, parts, part_width, rows), BF16),
        vmem((parts, part_width, rows), BF16),
        vmem((parts, part_width, rows), BF16),
        vmem((parts, 2, GROUP, rows, part_width), BF16),
        vmem((parts, tp_size, rows, part_width), BF16),
        vmem((tp_size, own_rows, 2 * HD), BF16),
        vmem((tp_size, own_rows, 2 * HD), BF16),
        vmem((parts, sides, depth, part_width), BF16),
        vmem((parts, sides, depth, part_width), BF16),
    ]
    sems = [
        pltpu.SemaphoreType.DMA,
        dma((tp_size,)),
        pltpu.SemaphoreType.DMA,
        dma((outer, tp_size)),
        dma((outer,)),
        dma((3,)),
        dma((3, GROUP)),
        pltpu.SemaphoreType.DMA,
        pltpu.SemaphoreType.DMA,
        pltpu.SemaphoreType.DMA,
        pltpu.SemaphoreType.DMA,
        pltpu.SemaphoreType.DMA,
        dma((parts,)),
        pltpu.SemaphoreType.DMA,
        dma((sides, 2)),
        pltpu.SemaphoreType.DMA,
        dma((parts + 1,)),
        pltpu.SemaphoreType.DMA,
        dma((parts,)),
        dma((2,)),
        dma((parts, 4)),
        pltpu.SemaphoreType.DMA,
        pltpu.SemaphoreType.DMA,
        pltpu.SemaphoreType.DMA,
        pltpu.SemaphoreType.DMA,
        pltpu.SemaphoreType.DMA,
        dma((parts,)),
        pltpu.SemaphoreType.DMA,
        pltpu.SemaphoreType.DMA,
        pltpu.SemaphoreType.DMA,
        dma((CHUNKS,)),
        pltpu.SemaphoreType.DMA,
        pltpu.SemaphoreType.DMA,
        dma((9,)),
    ]
    spec = pl.BlockSpec(memory_space=pl.ANY)
    held = pl.pallas_call(
        functools.partial(kernel, sp_size, tp_size),
        out_shape=(
            pltpu.VMEM((rows, d), BF16),
            pltpu.VMEM((own_rows, d), F32),
            pltpu.VMEM((depth, width), F32),
        ),
        in_specs=[spec] * 9,
        out_specs=(pl.BlockSpec(memory_space=pltpu.VMEM),) * 3,
        scratch_shapes=scratch + sems,
        compiler_params=pltpu.CompilerParams(
            collective_id=0, has_side_effects=True, vmem_limit_bytes=60000 * 1024
        ),
    )(
        *[
            pltpu.with_memory_space_constraint(x, pltpu.HBM)
            for x in (
                target,
                source,
                target_gain.reshape(1, d),
                source_gain.reshape(1, d),
                w_query,
                w_key,
                w_value,
                attended,
                d_attended,
            )
        ]
    )

    return pl.pallas_call(
        store_kernel,
        out_shape=(
            jax.ShapeDtypeStruct((rows, d), BF16),
            jax.ShapeDtypeStruct((own_rows, d), F32),
            jax.ShapeDtypeStruct((depth, width), F32),
        ),
        in_specs=[pl.BlockSpec(memory_space=pltpu.VMEM)] * 3,
        out_specs=(spec,) * 3,
        scratch_shapes=[dma((3,))],
    )(*[pltpu.with_memory_space_constraint(x, pltpu.VMEM) for x in held])


def store_kernel(a, b, c, a_h, b_h, c_h, sem):
    stores = [
        pltpu.make_async_copy(src, dst, sem.at[n])
        for n, (src, dst) in enumerate(((a, a_h), (b, b_h), (c, c_h)))
    ]
    for store in stores:
        store.start()
    for store in stores:
        store.wait()


def solution(mesh):
    return jax.shard_map(
        local,
        mesh=mesh,
        in_specs=(
            P("sp", None),
            P(("sp", "tp"), None),
            P(),
            P(),
            P(None, "tp"),
            P(),
            P(),
            P("sp", "tp"),
            P("sp", "tp"),
        ),
        out_specs=(P("sp", None), P(("sp", "tp"), None), P("sp", "tp")),
        check_vma=False,
    )
```

```python
import functools

import jax
import jax.numpy as jnp
from jax import lax
from jax.experimental import pallas as pl
from jax.experimental.pallas import tpu as pltpu
from jax.sharding import PartitionSpec as P

KVH = 2
HD = 128
EPS = 1e-06
GROUP = 4
CHUNKS = 4
LOG2E = 1.4426950408889634
MESH = pl.DeviceIdType.MESH
F32 = jnp.float32
BF16 = jnp.bfloat16

NT_DIMS = (((1,), (1,)), ((), ()))


def dot_nn(a, b):
    return jnp.dot(a, b, preferred_element_type=F32)


def dot_nt(a, b):
    return lax.dot_general(a, b, NT_DIMS, preferred_element_type=F32)


def inverse_rms(x):
    return lax.rsqrt(jnp.mean(x * x, axis=-1, keepdims=True) + EPS)


def norm_back(x, gain, cotangent):
    inv = inverse_rms(x)
    gc = cotangent * gain
    inner = jnp.mean(x * gc, axis=-1, keepdims=True)
    return inv * gc - x * (inv * inv * inv * inner)


def kernel(
    sp_size,
    tp_size,
    target_h,
    source_h,
    tgain_h,
    sgain_h,
    wq_h,
    wk_h,
    wv_h,
    att_h,
    dout_h,
    dtarget,
    dsource,
    dwq,
    target,
    source,
    tgain,
    sgain,
    wq,
    wk,
    wv,
    att,
    kvown,
    kvg,
    ktg,
    qg,
    og,
    qt,
    ot,
    delta,
    ntt,
    nttg,
    eb,
    pb,
    cmax,
    mrun,
    lrun,
    stat,
    psend,
    pget,
    dks,
    dkg,
    dkown,
    dkm,
    dkz,
    dqacc,
    dqs,
    dqr,
    dqm,
    dqz,
    dqg,
    dqx,
    rets,
    ret,
    dws,
    dwg,
    tkv_s,
    tkv_r,
    lkv_s,
    lkv_r,
    rl_s,
    in_s,
    in_r,
    nt_s,
    nt_r,
    st_s,
    st_r,
    ps_s,
    ps_r,
    dk_s,
    dk_r,
    dc_s,
    dc_r,
    dy_s,
    dy_r,
    ag_s,
    ag_r,
    rt_s,
    rt_r,
    dx_s,
    dx_r,
    dw_s,
    dw_r,
    dz_s,
    dz_r,
    wx_s,
    wx_r,
    wf_s,
    wf_r,
    ld_s,
):
    outer = sp_size // GROUP
    rows = target.shape[0]
    width = wq.shape[2]
    heads = width // HD
    own_rows = source.shape[0]
    block = own_rows * tp_size
    group_rows = GROUP * rows
    scaling = HD ** (-0.5)
    sp = lax.axis_index("sp")
    t = lax.axis_index("tp")
    z = sp // GROUP
    g = sp % GROUP
    per_kv = tp_size // KVH
    sides = outer // 2
    side = z // 2
    par = lax.rem(z, 2)
    zp = z + 1 - 2 * par
    parts = wq_parts(heads)
    part_heads = heads // parts
    part_width = width // parts
    chunk = wq.shape[1] // (2 * CHUNKS)

    def tp_peer(o):
        return lax.rem(t + o, tp_size)

    def z_peer(o):
        return lax.rem(z + o, outer)

    def to_tp(p):
        return {"sp": sp, "tp": p}

    def to_g(p):
        return {"sp": z * GROUP + p, "tp": t}

    def to_z(p):
        return {"sp": p * GROUP + g, "tp": t}

    def copy(src, dst, ssem, rsem, dev):
        return pltpu.make_async_remote_copy(
            src_ref=src, dst_ref=dst, send_sem=ssem, recv_sem=rsem, device_id=dev, device_id_type=MESH
        )

    def all_sent(ref, sem):
        copy(ref, ref, sem, sem, to_g(ga)).wait_send()

    def all_here(ref, sem):
        copy(ref, ref, sem, sem, to_g(ga)).wait_recv()

    odd = lax.rem(g, 2)
    ga = g + 1 - 2 * odd
    gb = lax.rem(g + 2, GROUP)
    gc = lax.rem(ga + 2, GROUP)
    near = (g, ga, gb, gc)

    loads = [
        pltpu.make_async_copy(src, dst, ld_s.at[n])
        for n, (src, dst) in enumerate(
            (
                (dout_h, og.at[0]),
                (source_h, source),
                (sgain_h, sgain),
                (wk_h, wk),
                (wv_h, wv),
                (target_h, target),
                (tgain_h, tgain),
                (wq_h, wq.at[t]),
                (att_h, att),
            )
        )
    ]
    for load in loads:
        load.start()

    barrier = pltpu.get_barrier_semaphore()
    for o in range(1, tp_size):
        pl.semaphore_signal(barrier, inc=1, device_id=to_tp(tp_peer(o)), device_id_type=MESH)
    for p in near[1:]:
        pl.semaphore_signal(barrier, inc=1, device_id=to_g(p), device_id_type=MESH)
    for p in near[1:]:
        pl.semaphore_signal(barrier, inc=1, device_id={"sp": zp * GROUP + p, "tp": t}, device_id_type=MESH)
    for o in range(1, outer):
        pl.semaphore_signal(barrier, inc=1, device_id=to_z(z_peer(o)), device_id_type=MESH)

    def group_copy(k, way, slot, there):
        ref = (og, qg, delta)[k]
        shared = max(k, 1) if there != 2 else k
        return copy(
            ref.at[slot], ref.at[there], in_s.at[k], in_r.at[shared, there], to_g((ga, gb, ga)[way])
        )

    def group_here(r):
        all_here(og.at[0:2], in_r.at[1, r])
        all_here(delta.at[0], in_r.at[2, r])

    def send_own(k):
        group_copy(k, 1, 0, 2).start()
        group_copy(k, 0, 0, 1).start()

    def forward(k):
        group_copy(k, 1, 0, 2).wait_recv()
        group_copy(k, 2, 2, 3).start()

    def enter():
        loads[0].wait()
        pl.semaphore_wait(barrier, tp_size + 2 * GROUP + outer - 4)
        send_own(0)

    pl.when(z == outer - 1)(enter)
    for n in range(1, 5):
        loads[n].wait()
    s32 = source[...].astype(F32)
    ns = (s32 * inverse_rms(s32) * sgain[...]).astype(BF16)
    keys = dot_nn(ns, wk[...]).astype(BF16)
    values = dot_nn(ns, wv[...]).astype(BF16)
    for c in range(KVH):
        kvown[c, :, 0:HD] = keys[:, c * HD : (c + 1) * HD]
        kvown[c, :, HD : 2 * HD] = values[:, c * HD : (c + 1) * HD]
    kvg[z, t] = kvown[t // per_kv]
    pl.when(z < outer - 1)(enter)

    def tkv(p, slot):
        return copy(kvown.at[p // per_kv], kvg.at[z, slot], tkv_s, tkv_r.at[slot], to_tp(p))

    def lkv(p, zslot, tslot):
        return copy(
            kvg.at[z, tslot], kvg.at[zslot, tslot], lkv_s, lkv_r.at[zslot, tslot], to_z(p)
        )

    def relay(zslot, tslot):
        ref = kvg.at[zslot, tslot]
        return copy(ref, ref, rl_s.at[zslot], lkv_r.at[zslot, tslot], to_z(zp))

    def each_rep(act):
        act(zp)
        for o in range(1, sides):
            p = lax.rem(side + o, sides)
            act(jnp.where(p > side, 2 * p, 2 * p + 1))

    def each_relay(dist, act):
        @pl.when((par == 0) & (z >= dist))
        def _():
            act(z - dist)

        @pl.when((par == 1) & (z + dist < outer))
        def _():
            act(z + dist)

    def pass_on(dist, ts):
        def act(p):
            lkv(p, p, ts).wait_recv()
            relay(p, ts).start()

        each_relay(dist, act)

    for o in range(1, tp_size):
        tkv(tp_peer(o), t).start()
    each_rep(lambda p: lkv(p, z, t).start())

    for n in range(5, 9):
        loads[n].wait()
    t32 = target[...].astype(F32)
    nt32 = t32 * inverse_rms(t32) * tgain[...]
    qg[0] = dot_nn(nt32.astype(BF16), wq[t]).astype(BF16)
    send_own(1)

    def half(slot, side, i):
        return wq.at[slot, pl.ds((side * CHUNKS + i) * chunk, chunk)]

    def wx_copy(p, slot, i):
        ref = half(slot, odd, i)
        return copy(ref, ref, wx_s, wx_r.at[i], to_tp(p))

    def wf_copy(slot, side, i):
        ref = half(slot, side, i)
        return copy(ref, ref, wf_s, wf_r, to_g(ga))

    prod = (og[0].astype(F32) * att[...].astype(F32)).T
    drows = [jnp.sum(prod[h * HD : (h + 1) * HD], axis=0, keepdims=True) for h in range(heads)]
    drows.append(jnp.zeros((8 - heads, rows), F32))
    delta[0] = jnp.concatenate(drows, axis=0).astype(BF16).astype(F32)
    send_own(2)

    def columns_copy(zr, r):
        layer = (z, zp)[zr]
        p = near[r]
        return copy(
            ntt.at[:, lax.rem(layer, 2), p],
            nttg.at[zr * GROUP + r],
            nt_s,
            nt_r,
            {"sp": layer * GROUP + p, "tp": t},
        )

    ntt[...] = nt32.T.astype(BF16).reshape(ntt.shape)
    nttg[0] = ntt[:, par, g]
    for o in range(1, tp_size):
        p = tp_peer(o)
        tkv(t, p).wait_recv()
        each_rep(lambda pz: lkv(pz, z, p).start())
    for i in range(CHUNKS):
        for o in range(1, tp_size):
            wx_copy(tp_peer(o), t, i).start()
    group_here(1)

    def turned(blocks):
        for r in blocks:
            for h in range(heads):
                cut = slice(h * group_rows + r * rows, h * group_rows + (r + 1) * rows)
                qt[:, cut] = qg[r, :, h * HD : (h + 1) * HD].astype(F32).T.astype(BF16)
                ot[:, cut] = og[r, :, h * HD : (h + 1) * HD].astype(F32).T.astype(BF16)

    turned((0, 1))
    mrun[...] = jnp.full(mrun.shape, -jnp.inf, F32)
    lrun[...] = jnp.zeros(lrun.shape, F32)
    dqacc[...] = jnp.zeros(dqacc.shape, F32)

    low = jnp.minimum(z, outer - 1 - z)

    def in_turn(o):
        pos = jnp.where(o <= low, low - o, o)
        return jnp.where(z == low, pos, outer - 1 - pos)

    def key_turn(zc):
        ktg[zc] = kvg[zc, :, :, 0:HD].reshape(block, HD).astype(F32).T.astype(BF16)

    half_rows = group_rows // 2
    steep = scaling * LOG2E

    def score(tiles, done=None):
        def products(zc, h, side_of):
            cut = slice(h * group_rows + side_of * half_rows, h * group_rows + (side_of + 1) * half_rows)
            kb = kvg[zc, :, :, 0:HD].reshape(block, HD)
            vb = kvg[zc, :, :, HD : 2 * HD].reshape(block, HD)
            return dot_nn(kb, qt[:, cut]), dot_nn(vb, ot[:, cut])

        def gather(zc, h, side_of, cut, keep, p):
            dqacc[h, :, cut] = dqacc[h, :, cut] * keep + dot_nn(ktg[zc], p)
            if done is not None and side_of == 1:
                done(h)

        ready = products(*tiles[0])
        held = None
        for n, (zc, h, side_of) in enumerate(tiles):
            s, dw = ready
            if n + 1 < len(tiles):
                ready = products(*tiles[n + 1])
            cut = slice(side_of * half_rows, (side_of + 1) * half_rows)
            wide = slice(h * group_rows + side_of * half_rows, h * group_rows + (side_of + 1) * half_rows)
            m_old = mrun[h : h + 1, cut]
            m = jnp.maximum(m_old, jnp.max(s, axis=0, keepdims=True))
            e = jnp.exp2(s * steep - m * steep)
            keep = jnp.exp2((m_old - m) * steep)
            lrun[h : h + 1, cut] = lrun[h : h + 1, cut] * keep + jnp.sum(e, axis=0, keepdims=True)
            mrun[h : h + 1, cut] = m
            cmax[zc, h : h + 1, cut] = m
            drow = jnp.concatenate([delta[2 * side_of + i, h : h + 1, :] for i in range(2)], axis=1)
            short = e.astype(BF16)
            p = short * (dw - drow).astype(BF16)
            eb[zc, :, wide] = short
            pb[zc, :, wide] = p
            if held is not None:
                gather(*held)
            held = (zc, h, side_of, cut, keep, p)
        gather(*held)

    def arrive(zc):
        for ts in range(tp_size):
            lkv(zc, zc, ts).wait_recv()

    def waits(zc):
        relayed = ((par == 0) & (zc < z)) | ((par == 1) & (zc > z))

        @pl.when(jnp.logical_not(relayed))
        def _():
            arrive(zc)

    def tiles_of(zc, sides_of):
        return [(zc, h, side_of) for side_of in sides_of for h in range(heads)]

    later = [tp_peer(o) for o in range(1, tp_size)]

    pass_on(1, t)
    key_turn(z)
    score(tiles_of(z, (0,)))
    forward(0)
    pass_on(2, t)
    for p in later:
        pass_on(1, p)
    one = in_turn(1)
    waits(one)
    forward(1)
    forward(2)
    key_turn(one)
    score(tiles_of(one, (0,)))
    for p in later:
        pass_on(2, p)
    for dist in range(3, outer):
        for ts in range(tp_size):
            pass_on(dist, ts)
    for r in (3, 2, 1):
        columns_copy(0, r).start()
    for r in (3, 2, 0, 1):
        columns_copy(1, r).start()
    group_here(3)
    turned((2, 3))

    def first(o, _):
        zc = in_turn(o)
        waits(zc)
        key_turn(zc)
        score(tiles_of(zc, (0, 1)))
        return 0

    score(tiles_of(z, (1,)) + tiles_of(one, (1,)))
    lax.fori_loop(2, outer - 1, first, 0)
    last = in_turn(outer - 1)
    waits(last)
    key_turn(last)

    def dc_copy(k, n):
        return copy(dqs.at[k, (1, 3)[n]], dqr.at[n, k], dc_s, dc_r.at[k * n + n], to_g(ga))

    def ps_copy(k):
        return copy(psend.at[k], pget.at[k], ps_s, ps_r.at[k], to_g(ga))

    def stat_copy(r):
        return copy(stat.at[0], stat.at[r], st_s, st_r, to_g(near[r]))

    def release(h):
        k = h // part_heads
        hh = h % part_heads
        norm = scaling / lrun[h : h + 1, :]
        for r in range(GROUP):
            cut = slice(r * rows, (r + 1) * rows)
            dqs[k, r, hh * HD : (hh + 1) * HD] = (dqacc[h, :, cut] * norm[:, cut]).astype(BF16)
        if hh == part_heads - 1:
            part = range(k * part_heads, (k + 1) * part_heads)
            logs = [mrun[j : j + 1, :] * scaling + jnp.log(lrun[j : j + 1, :]) for j in part]
            psend[k] = jnp.concatenate(logs + [jnp.zeros((8 - part_heads, group_rows), F32)], axis=0)
            ps_copy(k).start()
            dc_copy(k, 1).start()
            dc_copy(k, 0).start()

    score([(last, h, side_of) for h in range(heads) for side_of in (0, 1)], release)
    stat[0] = jnp.concatenate(
        [psend[k, 0:part_heads] for k in range(parts)] + [jnp.zeros((8 - heads, group_rows), F32)], axis=0
    )
    for r in (3, 2, 1):
        stat_copy(r).start()

    def in_order(full, r):
        return [full[:, (j ^ r) * rows : ((j ^ r) + 1) * rows] for j in range(GROUP)]

    def dy_copy(k):
        return copy(dqm.at[k], dqz.at[k], dy_s, dy_r.at[k], to_g(gb))

    for k in range(parts):
        ps_copy(k).wait_recv()
        dc_copy(k, 1).wait_recv()
        mine = in_order(psend[k], 0)[2]
        pairs = in_order(pget[k], 1)[2]
        top = jnp.maximum(mine, pairs)
        own_w = jnp.exp(mine - top)
        pair_w = jnp.exp(pairs - top)
        inv = 1.0 / (own_w + pair_w)
        own_w = own_w * inv
        pair_w = pair_w * inv
        for hh in range(part_heads):
            cut = slice(hh * HD, (hh + 1) * HD)
            dqm[k, cut] = (
                dqs[k, 2, cut].astype(F32) * own_w[hh : hh + 1] + dqr[1, k, cut].astype(F32) * pair_w[hh : hh + 1]
            ).astype(BF16)
        dy_copy(k).start()

    all_here(stat.at[1:GROUP], st_r)
    totals = [jnp.concatenate(in_order(stat[r], r), axis=1) for r in range(GROUP)]
    top = jnp.maximum(jnp.maximum(totals[0], totals[1]), jnp.maximum(totals[2], totals[3]))
    log_total = top + jnp.log(sum(jnp.exp(v - top) for v in totals))

    def dk_copy(i, n):
        return copy(dks.at[i, n], dkg.at[i, n], dk_s, dk_r.at[i, n], to_z(zp))

    def side_peer(o):
        return lax.rem(side + o, sides)

    def dz_copy(p, slot, n):
        return copy(dkm.at[p, n], dkz.at[slot, n], dz_s, dz_r, to_z(2 * p + par))

    def source_grad(zc, put):
        factor = jnp.concatenate(
            [jnp.exp(cmax[zc, h : h + 1, :] * scaling - log_total[h : h + 1, :]) for h in range(heads)], axis=1
        )
        qf = (qt[...].astype(F32) * (factor * scaling)).astype(BF16)
        of = (ot[...].astype(F32) * factor).astype(BF16)
        dk = dot_nt(pb[zc], qf)
        dv = dot_nt(eb[zc], of)
        put(0, dk)
        put(1, dv)

    def other(i, send):
        def put(n, value):
            dks[i, n] = value.astype(BF16)

        source_grad(2 * i + 1 - par, put)
        if send:
            for n in range(2):
                dk_copy(i, n).start()

    def mine(i):
        def put(n, value):
            dkown[i, n] = value

        source_grad(2 * i + par, put)

    for o in range(1, sides):
        other(side_peer(o), True)

    ways = (
        (to_g(ga), (0, 0), (0, 1)),
        (to_g(gb), (0, 0), (0, 2)),
        (to_z(zp), (0, 0), (1, 0)),
        (to_g(ga), (0, 2), (0, 3)),
        (to_g(gb), (1, 0), (1, 2)),
        (to_g(ga), (1, 0), (1, 1)),
        (to_g(ga), (1, 2), (1, 3)),
    )

    def ag_copy(k, way):
        dev, (zf, rf), (zt, rt) = ways[way]
        arrival = {1: 0, 2: 1, 4: 2}.get(way, 3)
        return copy(dqg.at[k, zf, rf], dqg.at[k, zt, rt], ag_s.at[way // 4], ag_r.at[k, arrival], dev)

    def dx_copy(k, p, slot):
        return copy(dqg.at[k, 0, 0], dqx.at[k, slot], dx_s, dx_r, to_tp(p))

    all_here(dqr.at[0], dc_r.at[0])
    weights = [jnp.exp(v[:, 0:rows] - log_total[:, 0:rows]) for v in totals]
    far_w = weights[2] + weights[3]
    for k in range(parts):
        dy_copy(k).wait_recv()
        sums = []
        for hh in range(part_heads):
            h = k * part_heads + hh
            cut = slice(hh * HD, (hh + 1) * HD)
            sums.append(
                dqs[k, 0, cut].astype(F32) * weights[0][h : h + 1]
                + dqr[0, k, cut].astype(F32) * weights[1][h : h + 1]
                + dqz[k, cut].astype(F32) * far_w[h : h + 1]
            )
        dqg[k, 0, 0] = jnp.concatenate(sums, axis=0).T.astype(BF16)
        for way in (2, 1, 0):
            ag_copy(k, way).start()
        for o in range(1, tp_size):
            dx_copy(k, tp_peer(o), t).start()
    for o in range(1, sides):
        mine(side_peer(o))
    other(side, False)
    mine(side)

    def forward_wq(i):
        all_here(wq.at[0 : tp_size - 1, 0:chunk], wx_r.at[i])
        for o in range(1, tp_size):
            wf_copy(tp_peer(o), odd, i).start()

    for i in range(CHUNKS - 2):
        forward_wq(i)
    for o in range(1, sides):
        i = side_peer(o)
        for n in range(2):
            dk_copy(i, n).wait_recv()
            dkm[i, n] = (dkown[i, n] + dkg[i, n].astype(F32)).astype(BF16)
            dz_copy(i, side, n).start()
    for n in range(2):
        dk_copy(side, n).start()
    for k in range(parts):
        ag_copy(k, 2).wait_recv()
        ag_copy(k, 4).start()
        ag_copy(k, 5).start()
        ag_copy(k, 1).wait_recv()
        ag_copy(k, 3).start()

    def dw_copy(k, p, slot):
        return copy(dws.at[k, p], dwg.at[k, slot], dw_s, dw_r.at[k], to_z(2 * p + par))

    depth = ntt.shape[3]
    forward_wq(CHUNKS - 2)
    all_here(nttg.at[1 : 2 * GROUP], nt_r)
    lhs = jnp.concatenate(
        [nttg[n].reshape(sides * depth, rows) for n in range(2 * GROUP)], axis=1
    )

    def weight_grad(k):
        all_here(dqg.at[k, 0], ag_r.at[k, 3])
        term = dot_nn(lhs, dqg[k].reshape(2 * group_rows, part_width))
        dws[k] = term.astype(BF16).reshape(dws.shape[1:])
        for o in range(1, sides):
            dw_copy(k, side_peer(o), side).start()

    for k in range(parts):
        ag_copy(k, 4).wait_recv()
        ag_copy(k, 6).start()
        if k > 0:
            weight_grad(k - 1)
        if k == parts // 2:
            forward_wq(CHUNKS - 1)
    weight_grad(parts - 1)
    all_here(dkz.at[0 : sides - 1], dz_r)
    totals_kv = []
    for n in range(2):
        dk_copy(side, n).wait_recv()
        total = dkown[side, n] + dkg[side, n].astype(F32)
        for o in range(1, sides):
            p = side_peer(o)
            total = total + dkz[p, n].astype(F32)
        totals_kv.append(total)
    rets[...] = jnp.concatenate(totals_kv, axis=1).astype(BF16).reshape(rets.shape)

    def ret_copy(p, slot):
        return copy(rets.at[p], ret.at[slot], rt_s, rt_r, to_tp(p))

    for o in range(1, tp_size):
        ret_copy(tp_peer(o), t).start()
    ret[t] = rets[t]

    for k in range(parts):
        dqx[k, t] = dqg[k, 0, 0]
    all_here(dqx.at[:, 0 : tp_size - 1], dx_r)
    all_here(wq.at[0 : tp_size - 1, 0 : CHUNKS * chunk], wf_r)
    dn = jnp.zeros((rows, wq.shape[1]), F32)
    for p in range(tp_size):
        full = jnp.concatenate([dqx[k, p] for k in range(parts)], axis=1)
        dn = dn + dot_nt(full, wq[p])
    dtarget[...] = norm_back(target[...].astype(F32), tgain[...], dn).astype(BF16)

    all_here(ret.at[0 : tp_size - 1], rt_r)
    dns = jnp.zeros(source.shape, F32)
    for c in range(KVH):
        part = ret[c * per_kv].astype(F32)
        for k in range(1, per_kv):
            part = part + ret[c * per_kv + k].astype(F32)
        part = part.astype(BF16)
        dns = dns + dot_nt(part[:, 0:HD], wk[:, c * HD : (c + 1) * HD])
        dns = dns + dot_nt(part[:, HD : 2 * HD], wv[:, c * HD : (c + 1) * HD])
    dsource[...] = norm_back(source[...].astype(F32), sgain[...], dns)

    for k in range(parts):
        dw_total = dws[k, side].astype(F32)
        all_here(dwg.at[k, 0 : sides - 1], dw_r.at[k])
        for o in range(1, sides):
            p = side_peer(o)
            dw_total = dw_total + dwg[k, p].astype(F32)
        dwq[:, k * part_width : (k + 1) * part_width] = dw_total

    all_sent(kvg.at[0, 0 : tp_size - 1], tkv_s)
    all_sent(kvg.at[0:sides], lkv_s)
    for dist in range(1, outer):
        each_relay(dist, lambda p: all_sent(kvg.at[p], rl_s.at[p]))
    all_sent(rets.at[0 : tp_size - 1], rt_s)
    all_sent(dqx.at[:, 0 : tp_size - 1], dx_s)
    all_sent(wq.at[0 : tp_size - 1, 0 : CHUNKS * chunk], wx_s)
    all_sent(wq.at[0 : tp_size - 1, 0 : CHUNKS * chunk], wf_s)
    for k, ref in enumerate((og, qg, delta)):
        all_sent(ref.at[0:3], in_s.at[k])
    all_sent(nttg.at[1 : 2 * GROUP], nt_s)
    all_sent(stat.at[1:GROUP], st_s)
    all_sent(psend, ps_s)
    all_sent(dqr, dc_s)
    all_sent(dqm, dy_s)
    all_sent(dqg.at[:, 0], ag_s.at[0])
    all_sent(dqg.at[:, 0, 0:3], ag_s.at[1])
    all_sent(dks, dk_s)
    all_sent(dkm.at[0 : sides - 1], dz_s)
    all_sent(dws.at[:, 0 : sides - 1], dw_s)


def wq_parts(heads):
    return heads


def local(target, source, target_gain, source_gain, w_query, w_key, w_value, attended, d_attended):
    sp_size = lax.axis_size("sp")
    tp_size = lax.axis_size("tp")
    outer = sp_size // GROUP
    sides = outer // 2
    rows, d = target.shape
    own_rows = source.shape[0]
    block = own_rows * tp_size
    width = w_query.shape[1]
    heads = width // HD
    depth = d // sp_size
    group_rows = GROUP * rows
    vmem = pltpu.VMEM
    dma = pltpu.SemaphoreType.DMA
    parts = wq_parts(heads)
    part_width = width // parts
    scratch = [
        vmem((rows, d), BF16),
        vmem((own_rows, d), BF16),
        vmem((1, d), F32),
        vmem((1, d), F32),
        vmem((tp_size, d, width), BF16),
        vmem(w_key.shape, BF16),
        vmem(w_value.shape, BF16),
        vmem((rows, width), BF16),
        vmem((KVH, own_rows, 2 * HD), BF16),
        vmem((outer, tp_size, own_rows, 2 * HD), BF16),
        vmem((outer, HD, block), BF16),
        vmem((GROUP, rows, width), BF16),
        vmem((GROUP, rows, width), BF16),
        vmem((HD, heads * group_rows), BF16),
        vmem((HD, heads * group_rows), BF16),
        vmem((GROUP, 8, rows), F32),
        vmem((sides, 2, GROUP, depth, rows), BF16),
        vmem((2 * GROUP, sides, depth, rows), BF16),
        vmem((outer, block, heads * group_rows), BF16),
        vmem((outer, block, heads * group_rows), BF16),
        vmem((outer, 8, group_rows), F32),
        vmem((8, group_rows), F32),
        vmem((8, group_rows), F32),
        vmem((GROUP, 8, group_rows), F32),
        vmem((parts, 8, group_rows), F32),
        vmem((parts, 8, group_rows), F32),
        vmem((sides, 2, block, HD), BF16),
        vmem((sides, 2, block, HD), BF16),
        vmem((sides, 2, block, HD), F32),
        vmem((sides, 2, block, HD), BF16),
        vmem((sides, 2, block, HD), BF16),
        vmem((heads, HD, group_rows), F32),
        vmem((parts, GROUP, part_width, rows), BF16),
        vmem((2, parts, part_width, rows), BF16),
        vmem((parts, part_width, rows), BF16),
        vmem((parts, part_width, rows), BF16),
        vmem((parts, 2, GROUP, rows, part_width), BF16),
        vmem((parts, tp_size, rows, part_width), BF16),
        vmem((tp_size, own_rows, 2 * HD), BF16),
        vmem((tp_size, own_rows, 2 * HD), BF16),
        vmem((parts, sides, depth, part_width), BF16),
        vmem((parts, sides, depth, part_width), BF16),
    ]
    sems = [
        pltpu.SemaphoreType.DMA,
        dma((tp_size,)),
        pltpu.SemaphoreType.DMA,
        dma((outer, tp_size)),
        dma((outer,)),
        dma((3,)),
        dma((3, GROUP)),
        pltpu.SemaphoreType.DMA,
        pltpu.SemaphoreType.DMA,
        pltpu.SemaphoreType.DMA,
        pltpu.SemaphoreType.DMA,
        pltpu.SemaphoreType.DMA,
        dma((parts,)),
        pltpu.SemaphoreType.DMA,
        dma((sides, 2)),
        pltpu.SemaphoreType.DMA,
        dma((parts + 1,)),
        pltpu.SemaphoreType.DMA,
        dma((parts,)),
        dma((2,)),
        dma((parts, 4)),
        pltpu.SemaphoreType.DMA,
        pltpu.SemaphoreType.DMA,
        pltpu.SemaphoreType.DMA,
        pltpu.SemaphoreType.DMA,
        pltpu.SemaphoreType.DMA,
        dma((parts,)),
        pltpu.SemaphoreType.DMA,
        pltpu.SemaphoreType.DMA,
        pltpu.SemaphoreType.DMA,
        dma((CHUNKS,)),
        pltpu.SemaphoreType.DMA,
        pltpu.SemaphoreType.DMA,
        dma((9,)),
    ]
    spec = pl.BlockSpec(memory_space=pl.ANY)
    held = pl.pallas_call(
        functools.partial(kernel, sp_size, tp_size),
        out_shape=(
            pltpu.VMEM((rows, d), BF16),
            pltpu.VMEM((own_rows, d), F32),
            pltpu.VMEM((depth, width), F32),
        ),
        in_specs=[spec] * 9,
        out_specs=(pl.BlockSpec(memory_space=pltpu.VMEM),) * 3,
        scratch_shapes=scratch + sems,
        compiler_params=pltpu.CompilerParams(
            collective_id=0, has_side_effects=True, vmem_limit_bytes=60000 * 1024
        ),
    )(
        *[
            pltpu.with_memory_space_constraint(x, pltpu.HBM)
            for x in (
                target,
                source,
                target_gain.reshape(1, d),
                source_gain.reshape(1, d),
                w_query,
                w_key,
                w_value,
                attended,
                d_attended,
            )
        ]
    )

    return pl.pallas_call(
        store_kernel,
        out_shape=(
            jax.ShapeDtypeStruct((rows, d), BF16),
            jax.ShapeDtypeStruct((own_rows, d), F32),
            jax.ShapeDtypeStruct((depth, width), F32),
        ),
        in_specs=[pl.BlockSpec(memory_space=pltpu.VMEM)] * 3,
        out_specs=(spec,) * 3,
        scratch_shapes=[dma((3,))],
    )(*[pltpu.with_memory_space_constraint(x, pltpu.VMEM) for x in held])


def store_kernel(a, b, c, a_h, b_h, c_h, sem):
    stores = [
        pltpu.make_async_copy(src, dst, sem.at[n])
        for n, (src, dst) in enumerate(((a, a_h), (b, b_h), (c, c_h)))
    ]
    for store in stores:
        store.start()
    for store in stores:
        store.wait()


def solution(mesh):
    return jax.shard_map(
        local,
        mesh=mesh,
        in_specs=(
            P("sp", None),
            P(("sp", "tp"), None),
            P(),
            P(),
            P(None, "tp"),
            P(),
            P(),
            P("sp", "tp"),
            P("sp", "tp"),
        ),
        out_specs=(P("sp", None), P(("sp", "tp"), None), P("sp", "tp")),
        check_vma=False,
    )
```

```python
import functools

import jax
import jax.numpy as jnp
from jax import lax
from jax.experimental import pallas as pl
from jax.experimental.pallas import tpu as pltpu
from jax.sharding import PartitionSpec as P

KVH = 2
HD = 128
EPS = 1e-06
GROUP = 4
CHUNKS = 4
LOG2E = 1.4426950408889634
MESH = pl.DeviceIdType.MESH
F32 = jnp.float32
BF16 = jnp.bfloat16

NT_DIMS = (((1,), (1,)), ((), ()))


def dot_nn(a, b):
    return jnp.dot(a, b, preferred_element_type=F32)


def dot_nt(a, b):
    return lax.dot_general(a, b, NT_DIMS, preferred_element_type=F32)


def inverse_rms(x):
    return lax.rsqrt(jnp.mean(x * x, axis=-1, keepdims=True) + EPS)


def norm_back(x, gain, cotangent):
    inv = inverse_rms(x)
    gc = cotangent * gain
    inner = jnp.mean(x * gc, axis=-1, keepdims=True)
    return inv * gc - x * (inv * inv * inv * inner)


def kernel(
    sp_size,
    tp_size,
    target_h,
    source_h,
    tgain_h,
    sgain_h,
    wq_h,
    wk_h,
    wv_h,
    att_h,
    dout_h,
    dtarget,
    dsource,
    dwq,
    target,
    source,
    tgain,
    sgain,
    wq,
    wk,
    wv,
    att,
    kvown,
    kvg,
    ktg,
    qg,
    og,
    qt,
    ot,
    delta,
    ntt,
    nttg,
    eb,
    pb,
    cmax,
    mrun,
    lrun,
    stat,
    psend,
    pget,
    dks,
    dkg,
    dkown,
    dkm,
    dkz,
    dqacc,
    dqs,
    dqr,
    dqm,
    dqz,
    dqg,
    dqx,
    rets,
    ret,
    dws,
    dwg,
    tkv_s,
    tkv_r,
    lkv_s,
    lkv_r,
    rl_s,
    in_s,
    in_r,
    nt_s,
    nt_r,
    st_s,
    st_r,
    ps_s,
    ps_r,
    dk_s,
    dk_r,
    dc_s,
    dc_r,
    dy_s,
    dy_r,
    ag_s,
    ag_r,
    rt_s,
    rt_r,
    dx_s,
    dx_r,
    dw_s,
    dw_r,
    dz_s,
    dz_r,
    wx_s,
    wx_r,
    wf_s,
    wf_r,
    ld_s,
):
    outer = sp_size // GROUP
    rows = target.shape[0]
    width = wq.shape[2]
    heads = width // HD
    own_rows = source.shape[0]
    block = own_rows * tp_size
    group_rows = GROUP * rows
    scaling = HD ** (-0.5)
    sp = lax.axis_index("sp")
    t = lax.axis_index("tp")
    z = sp // GROUP
    g = sp % GROUP
    per_kv = tp_size // KVH
    sides = outer // 2
    side = z // 2
    par = lax.rem(z, 2)
    zp = z + 1 - 2 * par
    parts = wq_parts(heads)
    part_heads = heads // parts
    part_width = width // parts
    chunk = wq.shape[1] // (2 * CHUNKS)

    def tp_peer(o):
        return lax.rem(t + o, tp_size)

    def z_peer(o):
        return lax.rem(z + o, outer)

    def to_tp(p):
        return {"sp": sp, "tp": p}

    def to_g(p):
        return {"sp": z * GROUP + p, "tp": t}

    def to_z(p):
        return {"sp": p * GROUP + g, "tp": t}

    def copy(src, dst, ssem, rsem, dev):
        return pltpu.make_async_remote_copy(
            src_ref=src, dst_ref=dst, send_sem=ssem, recv_sem=rsem, device_id=dev, device_id_type=MESH
        )

    def all_sent(ref, sem):
        copy(ref, ref, sem, sem, to_g(ga)).wait_send()

    def all_here(ref, sem):
        copy(ref, ref, sem, sem, to_g(ga)).wait_recv()

    odd = lax.rem(g, 2)
    ga = g + 1 - 2 * odd
    gb = lax.rem(g + 2, GROUP)
    gc = lax.rem(ga + 2, GROUP)
    near = (g, ga, gb, gc)

    loads = [
        pltpu.make_async_copy(src, dst, ld_s.at[n])
        for n, (src, dst) in enumerate(
            (
                (dout_h, og.at[0]),
                (source_h, source),
                (sgain_h, sgain),
                (wk_h, wk),
                (wv_h, wv),
                (target_h, target),
                (tgain_h, tgain),
                (wq_h, wq.at[t]),
                (att_h, att),
            )
        )
    ]
    for load in loads:
        load.start()

    barrier = pltpu.get_barrier_semaphore()
    for o in range(1, tp_size):
        pl.semaphore_signal(barrier, inc=1, device_id=to_tp(tp_peer(o)), device_id_type=MESH)
    for p in near[1:]:
        pl.semaphore_signal(barrier, inc=1, device_id=to_g(p), device_id_type=MESH)
    for p in near[1:]:
        pl.semaphore_signal(barrier, inc=1, device_id={"sp": zp * GROUP + p, "tp": t}, device_id_type=MESH)
    for o in range(1, outer):
        pl.semaphore_signal(barrier, inc=1, device_id=to_z(z_peer(o)), device_id_type=MESH)

    def group_copy(k, way, slot, there):
        ref = (og, qg, delta)[k]
        shared = max(k, 1) if there != 2 else k
        return copy(
            ref.at[slot], ref.at[there], in_s.at[k], in_r.at[shared, there], to_g((ga, gb, ga)[way])
        )

    def group_here(r):
        all_here(og.at[0:2], in_r.at[1, r])
        all_here(delta.at[0], in_r.at[2, r])

    def send_own(k):
        group_copy(k, 1, 0, 2).start()
        group_copy(k, 0, 0, 1).start()

    def forward(k):
        group_copy(k, 1, 0, 2).wait_recv()
        group_copy(k, 2, 2, 3).start()

    def enter():
        loads[0].wait()
        pl.semaphore_wait(barrier, tp_size + 2 * GROUP + outer - 4)
        send_own(0)

    pl.when(z == outer - 1)(enter)
    for n in range(1, 5):
        loads[n].wait()
    s32 = source[...].astype(F32)
    ns = (s32 * inverse_rms(s32) * sgain[...]).astype(BF16)
    keys = dot_nn(ns, wk[...]).astype(BF16)
    values = dot_nn(ns, wv[...]).astype(BF16)
    for c in range(KVH):
        kvown[c, :, 0:HD] = keys[:, c * HD : (c + 1) * HD]
        kvown[c, :, HD : 2 * HD] = values[:, c * HD : (c + 1) * HD]
    kvg[z, t] = kvown[t // per_kv]
    pl.when(z < outer - 1)(enter)

    def tkv(p, slot):
        return copy(kvown.at[p // per_kv], kvg.at[z, slot], tkv_s, tkv_r.at[slot], to_tp(p))

    def lkv(p, zslot, tslot):
        return copy(
            kvg.at[z, tslot], kvg.at[zslot, tslot], lkv_s, lkv_r.at[zslot, tslot], to_z(p)
        )

    def relay(zslot, tslot):
        ref = kvg.at[zslot, tslot]
        return copy(ref, ref, rl_s.at[zslot], lkv_r.at[zslot, tslot], to_z(zp))

    def each_rep(act):
        act(zp)
        for o in range(1, sides):
            p = lax.rem(side + o, sides)
            act(jnp.where(p > side, 2 * p, 2 * p + 1))

    def each_relay(dist, act):
        @pl.when((par == 0) & (z >= dist))
        def _():
            act(z - dist)

        @pl.when((par == 1) & (z + dist < outer))
        def _():
            act(z + dist)

    def pass_on(dist, ts):
        def act(p):
            lkv(p, p, ts).wait_recv()
            relay(p, ts).start()

        each_relay(dist, act)

    for o in range(1, tp_size):
        tkv(tp_peer(o), t).start()
    each_rep(lambda p: lkv(p, z, t).start())

    for n in range(5, 9):
        loads[n].wait()
    t32 = target[...].astype(F32)
    nt32 = t32 * inverse_rms(t32) * tgain[...]
    qg[0] = dot_nn(nt32.astype(BF16), wq[t]).astype(BF16)
    send_own(1)

    def half(slot, side, i):
        return wq.at[slot, pl.ds((side * CHUNKS + i) * chunk, chunk)]

    def wx_copy(p, slot, i):
        ref = half(slot, odd, i)
        return copy(ref, ref, wx_s, wx_r.at[i], to_tp(p))

    def wf_copy(slot, side, i):
        ref = half(slot, side, i)
        return copy(ref, ref, wf_s, wf_r, to_g(ga))

    prod = (og[0].astype(F32) * att[...].astype(F32)).T
    drows = [jnp.sum(prod[h * HD : (h + 1) * HD], axis=0, keepdims=True) for h in range(heads)]
    drows.append(jnp.zeros((8 - heads, rows), F32))
    delta[0] = jnp.concatenate(drows, axis=0).astype(BF16).astype(F32)
    send_own(2)

    def columns_copy(zr, r):
        layer = (z, zp)[zr]
        p = near[r]
        return copy(
            ntt.at[:, lax.rem(layer, 2), p],
            nttg.at[zr * GROUP + r],
            nt_s,
            nt_r,
            {"sp": layer * GROUP + p, "tp": t},
        )

    ntt[...] = nt32.T.astype(BF16).reshape(ntt.shape)
    nttg[0] = ntt[:, par, g]
    for o in range(1, tp_size):
        p = tp_peer(o)
        tkv(t, p).wait_recv()
        each_rep(lambda pz: lkv(pz, z, p).start())
    for i in range(CHUNKS):
        for o in range(1, tp_size):
            wx_copy(tp_peer(o), t, i).start()
    group_here(1)

    def turned(blocks):
        for r in blocks:
            for h in range(heads):
                cut = slice(h * group_rows + r * rows, h * group_rows + (r + 1) * rows)
                qt[:, cut] = qg[r, :, h * HD : (h + 1) * HD].astype(F32).T.astype(BF16)
                ot[:, cut] = og[r, :, h * HD : (h + 1) * HD].astype(F32).T.astype(BF16)

    turned((0, 1))
    mrun[...] = jnp.full(mrun.shape, -jnp.inf, F32)
    lrun[...] = jnp.zeros(lrun.shape, F32)
    dqacc[...] = jnp.zeros(dqacc.shape, F32)

    low = jnp.minimum(z, outer - 1 - z)

    def in_turn(o):
        pos = jnp.where(o <= low, low - o, o)
        return jnp.where(z == low, pos, outer - 1 - pos)

    def key_turn(zc):
        ktg[zc] = kvg[zc, :, :, 0:HD].reshape(block, HD).astype(F32).T.astype(BF16)

    half_rows = group_rows // 2
    steep = scaling * LOG2E

    def score(tiles, done=None):
        def products(zc, h, side_of):
            cut = slice(h * group_rows + side_of * half_rows, h * group_rows + (side_of + 1) * half_rows)
            kb = kvg[zc, :, :, 0:HD].reshape(block, HD)
            vb = kvg[zc, :, :, HD : 2 * HD].reshape(block, HD)
            return dot_nn(kb, qt[:, cut]), dot_nn(vb, ot[:, cut])

        def gather(zc, h, side_of, cut, keep, p):
            dqacc[h, :, cut] = dqacc[h, :, cut] * keep + dot_nn(ktg[zc], p)
            if done is not None and side_of == 1:
                done(h)

        ready = products(*tiles[0])
        held = None
        for n, (zc, h, side_of) in enumerate(tiles):
            s, dw = ready
            if n + 1 < len(tiles):
                ready = products(*tiles[n + 1])
            cut = slice(side_of * half_rows, (side_of + 1) * half_rows)
            wide = slice(h * group_rows + side_of * half_rows, h * group_rows + (side_of + 1) * half_rows)
            m_old = mrun[h : h + 1, cut]
            m = jnp.maximum(m_old, jnp.max(s, axis=0, keepdims=True))
            e = jnp.exp2(s * steep - m * steep)
            keep = jnp.exp2((m_old - m) * steep)
            lrun[h : h + 1, cut] = lrun[h : h + 1, cut] * keep + jnp.sum(e, axis=0, keepdims=True)
            mrun[h : h + 1, cut] = m
            cmax[zc, h : h + 1, cut] = m
            drow = jnp.concatenate([delta[2 * side_of + i, h : h + 1, :] for i in range(2)], axis=1)
            short = e.astype(BF16)
            p = short * (dw - drow).astype(BF16)
            eb[zc, :, wide] = short
            pb[zc, :, wide] = p
            if held is not None:
                gather(*held)
            held = (zc, h, side_of, cut, keep, p)
        gather(*held)

    def arrive(zc):
        for ts in range(tp_size):
            lkv(zc, zc, ts).wait_recv()

    def waits(zc):
        relayed = ((par == 0) & (zc < z)) | ((par == 1) & (zc > z))

        @pl.when(jnp.logical_not(relayed))
        def _():
            arrive(zc)

    def tiles_of(zc, sides_of):
        return [(zc, h, side_of) for side_of in sides_of for h in range(heads)]

    later = [tp_peer(o) for o in range(1, tp_size)]

    pass_on(1, t)
    key_turn(z)
    score(tiles_of(z, (0,)))
    forward(0)
    pass_on(2, t)
    for p in later:
        pass_on(1, p)
    one = in_turn(1)
    waits(one)
    forward(1)
    forward(2)
    key_turn(one)
    score(tiles_of(one, (0,)))
    for p in later:
        pass_on(2, p)
    for dist in range(3, outer):
        for ts in range(tp_size):
            pass_on(dist, ts)
    for r in (3, 2, 1):
        columns_copy(0, r).start()
    for r in (3, 2, 0, 1):
        columns_copy(1, r).start()
    group_here(3)
    turned((2, 3))

    def first(o, _):
        zc = in_turn(o)
        waits(zc)
        key_turn(zc)
        score(tiles_of(zc, (0, 1)))
        return 0

    score(tiles_of(z, (1,)) + tiles_of(one, (1,)))
    lax.fori_loop(2, outer - 1, first, 0)
    last = in_turn(outer - 1)
    waits(last)
    key_turn(last)

    def dc_copy(k, n):
        return copy(dqs.at[k, (1, 3)[n]], dqr.at[n, k], dc_s, dc_r.at[k * n + n], to_g(ga))

    def ps_copy(k):
        return copy(psend.at[k], pget.at[k], ps_s, ps_r.at[k], to_g(ga))

    def stat_copy(r):
        return copy(stat.at[0], stat.at[r], st_s, st_r, to_g(near[r]))

    def release(h):
        k = h // part_heads
        hh = h % part_heads
        norm = scaling / lrun[h : h + 1, :]
        for r in range(GROUP):
            cut = slice(r * rows, (r + 1) * rows)
            dqs[k, r, hh * HD : (hh + 1) * HD] = (dqacc[h, :, cut] * norm[:, cut]).astype(BF16)
        if hh == part_heads - 1:
            part = range(k * part_heads, (k + 1) * part_heads)
            logs = [mrun[j : j + 1, :] * scaling + jnp.log(lrun[j : j + 1, :]) for j in part]
            psend[k] = jnp.concatenate(logs + [jnp.zeros((8 - part_heads, group_rows), F32)], axis=0)
            ps_copy(k).start()
            dc_copy(k, 1).start()
            dc_copy(k, 0).start()

    score([(last, h, side_of) for h in range(heads) for side_of in (0, 1)], release)
    stat[0] = jnp.concatenate(
        [psend[k, 0:part_heads] for k in range(parts)] + [jnp.zeros((8 - heads, group_rows), F32)], axis=0
    )
    for r in (3, 2, 1):
        stat_copy(r).start()

    def in_order(full, r):
        return [full[:, (j ^ r) * rows : ((j ^ r) + 1) * rows] for j in range(GROUP)]

    def dy_copy(k):
        return copy(dqm.at[k], dqz.at[k], dy_s, dy_r.at[k], to_g(gb))

    for k in range(parts):
        ps_copy(k).wait_recv()
        dc_copy(k, 1).wait_recv()
        mine = in_order(psend[k], 0)[2]
        pairs = in_order(pget[k], 1)[2]
        top = jnp.maximum(mine, pairs)
        own_w = jnp.exp(mine - top)
        pair_w = jnp.exp(pairs - top)
        inv = 1.0 / (own_w + pair_w)
        own_w = own_w * inv
        pair_w = pair_w * inv
        for hh in range(part_heads):
            cut = slice(hh * HD, (hh + 1) * HD)
            dqm[k, cut] = (
                dqs[k, 2, cut].astype(F32) * own_w[hh : hh + 1] + dqr[1, k, cut].astype(F32) * pair_w[hh : hh + 1]
            ).astype(BF16)
        dy_copy(k).start()

    all_here(stat.at[1:GROUP], st_r)
    totals = [jnp.concatenate(in_order(stat[r], r), axis=1) for r in range(GROUP)]
    top = jnp.maximum(jnp.maximum(totals[0], totals[1]), jnp.maximum(totals[2], totals[3]))
    log_total = top + jnp.log(sum(jnp.exp(v - top) for v in totals))

    def dk_copy(i, n):
        return copy(dks.at[i, n], dkg.at[i, n], dk_s, dk_r.at[i, n], to_z(zp))

    def side_peer(o):
        return lax.rem(side + o, sides)

    def dz_copy(p, slot, n):
        return copy(dkm.at[p, n], dkz.at[slot, n], dz_s, dz_r, to_z(2 * p + par))

    def source_grad(zc, put):
        factor = jnp.concatenate(
            [jnp.exp(cmax[zc, h : h + 1, :] * scaling - log_total[h : h + 1, :]) for h in range(heads)], axis=1
        )
        qf = (qt[...].astype(F32) * (factor * scaling)).astype(BF16)
        of = (ot[...].astype(F32) * factor).astype(BF16)
        dk = dot_nt(pb[zc], qf)
        dv = dot_nt(eb[zc], of)
        put(0, dk)
        put(1, dv)

    def other(i, send):
        def put(n, value):
            dks[i, n] = value.astype(BF16)

        source_grad(2 * i + 1 - par, put)
        if send:
            dk_copy(i, 0).start()

    def mine(i):
        def put(n, value):
            dkown[i, n] = value

        source_grad(2 * i + par, put)

    for o in range(1, sides):
        other(side_peer(o), True)

    ways = (
        (to_g(ga), (0, 0), (0, 1)),
        (to_g(gb), (0, 0), (0, 2)),
        (to_z(zp), (0, 0), (1, 0)),
        (to_g(ga), (0, 2), (0, 3)),
        (to_g(gb), (1, 0), (1, 2)),
        (to_g(ga), (1, 0), (1, 1)),
        (to_g(ga), (1, 2), (1, 3)),
    )

    def ag_copy(k, way):
        dev, (zf, rf), (zt, rt) = ways[way]
        arrival = {1: 0, 2: 1, 4: 2}.get(way, 3)
        return copy(dqg.at[k, zf, rf], dqg.at[k, zt, rt], ag_s.at[way // 4], ag_r.at[k, arrival], dev)

    def dx_copy(k, p, slot):
        return copy(dqg.at[k, 0, 0], dqx.at[k, slot], dx_s, dx_r, to_tp(p))

    all_here(dqr.at[0], dc_r.at[0])
    weights = [jnp.exp(v[:, 0:rows] - log_total[:, 0:rows]) for v in totals]
    far_w = weights[2] + weights[3]
    for k in range(parts):
        dy_copy(k).wait_recv()
        sums = []
        for hh in range(part_heads):
            h = k * part_heads + hh
            cut = slice(hh * HD, (hh + 1) * HD)
            sums.append(
                dqs[k, 0, cut].astype(F32) * weights[0][h : h + 1]
                + dqr[0, k, cut].astype(F32) * weights[1][h : h + 1]
                + dqz[k, cut].astype(F32) * far_w[h : h + 1]
            )
        dqg[k, 0, 0] = jnp.concatenate(sums, axis=0).T.astype(BF16)
        for way in (2, 1, 0):
            ag_copy(k, way).start()
        for o in range(1, tp_size):
            dx_copy(k, tp_peer(o), t).start()
    for o in range(1, sides):
        dk_copy(side_peer(o), 1).start()
    for o in range(1, sides):
        mine(side_peer(o))
    other(side, False)
    mine(side)

    def forward_wq(i):
        all_here(wq.at[0 : tp_size - 1, 0:chunk], wx_r.at[i])
        for o in range(1, tp_size):
            wf_copy(tp_peer(o), odd, i).start()

    for i in range(CHUNKS - 2):
        forward_wq(i)
    for o in range(1, sides):
        i = side_peer(o)
        for n in range(2):
            dk_copy(i, n).wait_recv()
            dkm[i, n] = (dkown[i, n] + dkg[i, n].astype(F32)).astype(BF16)
            dz_copy(i, side, n).start()
    for n in range(2):
        dk_copy(side, n).start()
    for k in range(parts):
        ag_copy(k, 2).wait_recv()
        ag_copy(k, 4).start()
        ag_copy(k, 5).start()
        ag_copy(k, 1).wait_recv()
        ag_copy(k, 3).start()

    def dw_copy(k, p, slot):
        return copy(dws.at[k, p], dwg.at[k, slot], dw_s, dw_r.at[k], to_z(2 * p + par))

    depth = ntt.shape[3]
    forward_wq(CHUNKS - 2)
    all_here(nttg.at[1 : 2 * GROUP], nt_r)
    lhs = jnp.concatenate(
        [nttg[n].reshape(sides * depth, rows) for n in range(2 * GROUP)], axis=1
    )

    def weight_grad(k):
        all_here(dqg.at[k, 0], ag_r.at[k, 3])
        term = dot_nn(lhs, dqg[k].reshape(2 * group_rows, part_width))
        dws[k] = term.astype(BF16).reshape(dws.shape[1:])
        for o in range(1, sides):
            dw_copy(k, side_peer(o), side).start()

    for k in range(parts):
        ag_copy(k, 4).wait_recv()
        ag_copy(k, 6).start()
        if k > 0:
            weight_grad(k - 1)
        if k == parts // 2:
            forward_wq(CHUNKS - 1)
    weight_grad(parts - 1)
    all_here(dkz.at[0 : sides - 1], dz_r)
    totals_kv = []
    for n in range(2):
        dk_copy(side, n).wait_recv()
        total = dkown[side, n] + dkg[side, n].astype(F32)
        for o in range(1, sides):
            p = side_peer(o)
            total = total + dkz[p, n].astype(F32)
        totals_kv.append(total)
    rets[...] = jnp.concatenate(totals_kv, axis=1).astype(BF16).reshape(rets.shape)

    def ret_copy(p, slot):
        return copy(rets.at[p], ret.at[slot], rt_s, rt_r, to_tp(p))

    for o in range(1, tp_size):
        ret_copy(tp_peer(o), t).start()
    ret[t] = rets[t]

    for k in range(parts):
        dqx[k, t] = dqg[k, 0, 0]
    all_here(dqx.at[:, 0 : tp_size - 1], dx_r)
    all_here(wq.at[0 : tp_size - 1, 0 : CHUNKS * chunk], wf_r)
    dn = jnp.zeros((rows, wq.shape[1]), F32)
    for p in range(tp_size):
        full = jnp.concatenate([dqx[k, p] for k in range(parts)], axis=1)
        dn = dn + dot_nt(full, wq[p])
    dtarget[...] = norm_back(target[...].astype(F32), tgain[...], dn).astype(BF16)

    all_here(ret.at[0 : tp_size - 1], rt_r)
    dns = jnp.zeros(source.shape, F32)
    for c in range(KVH):
        part = ret[c * per_kv].astype(F32)
        for k in range(1, per_kv):
            part = part + ret[c * per_kv + k].astype(F32)
        part = part.astype(BF16)
        dns = dns + dot_nt(part[:, 0:HD], wk[:, c * HD : (c + 1) * HD])
        dns = dns + dot_nt(part[:, HD : 2 * HD], wv[:, c * HD : (c + 1) * HD])
    dsource[...] = norm_back(source[...].astype(F32), sgain[...], dns)

    for k in range(parts):
        dw_total = dws[k, side].astype(F32)
        all_here(dwg.at[k, 0 : sides - 1], dw_r.at[k])
        for o in range(1, sides):
            p = side_peer(o)
            dw_total = dw_total + dwg[k, p].astype(F32)
        dwq[:, k * part_width : (k + 1) * part_width] = dw_total

    all_sent(kvg.at[0, 0 : tp_size - 1], tkv_s)
    all_sent(kvg.at[0:sides], lkv_s)
    for dist in range(1, outer):
        each_relay(dist, lambda p: all_sent(kvg.at[p], rl_s.at[p]))
    all_sent(rets.at[0 : tp_size - 1], rt_s)
    all_sent(dqx.at[:, 0 : tp_size - 1], dx_s)
    all_sent(wq.at[0 : tp_size - 1, 0 : CHUNKS * chunk], wx_s)
    all_sent(wq.at[0 : tp_size - 1, 0 : CHUNKS * chunk], wf_s)
    for k, ref in enumerate((og, qg, delta)):
        all_sent(ref.at[0:3], in_s.at[k])
    all_sent(nttg.at[1 : 2 * GROUP], nt_s)
    all_sent(stat.at[1:GROUP], st_s)
    all_sent(psend, ps_s)
    all_sent(dqr, dc_s)
    all_sent(dqm, dy_s)
    all_sent(dqg.at[:, 0], ag_s.at[0])
    all_sent(dqg.at[:, 0, 0:3], ag_s.at[1])
    all_sent(dks, dk_s)
    all_sent(dkm.at[0 : sides - 1], dz_s)
    all_sent(dws.at[:, 0 : sides - 1], dw_s)


def wq_parts(heads):
    return heads


def local(target, source, target_gain, source_gain, w_query, w_key, w_value, attended, d_attended):
    sp_size = lax.axis_size("sp")
    tp_size = lax.axis_size("tp")
    outer = sp_size // GROUP
    sides = outer // 2
    rows, d = target.shape
    own_rows = source.shape[0]
    block = own_rows * tp_size
    width = w_query.shape[1]
    heads = width // HD
    depth = d // sp_size
    group_rows = GROUP * rows
    vmem = pltpu.VMEM
    dma = pltpu.SemaphoreType.DMA
    parts = wq_parts(heads)
    part_width = width // parts
    scratch = [
        vmem((rows, d), BF16),
        vmem((own_rows, d), BF16),
        vmem((1, d), F32),
        vmem((1, d), F32),
        vmem((tp_size, d, width), BF16),
        vmem(w_key.shape, BF16),
        vmem(w_value.shape, BF16),
        vmem((rows, width), BF16),
        vmem((KVH, own_rows, 2 * HD), BF16),
        vmem((outer, tp_size, own_rows, 2 * HD), BF16),
        vmem((outer, HD, block), BF16),
        vmem((GROUP, rows, width), BF16),
        vmem((GROUP, rows, width), BF16),
        vmem((HD, heads * group_rows), BF16),
        vmem((HD, heads * group_rows), BF16),
        vmem((GROUP, 8, rows), F32),
        vmem((sides, 2, GROUP, depth, rows), BF16),
        vmem((2 * GROUP, sides, depth, rows), BF16),
        vmem((outer, block, heads * group_rows), BF16),
        vmem((outer, block, heads * group_rows), BF16),
        vmem((outer, 8, group_rows), F32),
        vmem((8, group_rows), F32),
        vmem((8, group_rows), F32),
        vmem((GROUP, 8, group_rows), F32),
        vmem((parts, 8, group_rows), F32),
        vmem((parts, 8, group_rows), F32),
        vmem((sides, 2, block, HD), BF16),
        vmem((sides, 2, block, HD), BF16),
        vmem((sides, 2, block, HD), F32),
        vmem((sides, 2, block, HD), BF16),
        vmem((sides, 2, block, HD), BF16),
        vmem((heads, HD, group_rows), F32),
        vmem((parts, GROUP, part_width, rows), BF16),
        vmem((2, parts, part_width, rows), BF16),
        vmem((parts, part_width, rows), BF16),
        vmem((parts, part_width, rows), BF16),
        vmem((parts, 2, GROUP, rows, part_width), BF16),
        vmem((parts, tp_size, rows, part_width), BF16),
        vmem((tp_size, own_rows, 2 * HD), BF16),
        vmem((tp_size, own_rows, 2 * HD), BF16),
        vmem((parts, sides, depth, part_width), BF16),
        vmem((parts, sides, depth, part_width), BF16),
    ]
    sems = [
        pltpu.SemaphoreType.DMA,
        dma((tp_size,)),
        pltpu.SemaphoreType.DMA,
        dma((outer, tp_size)),
        dma((outer,)),
        dma((3,)),
        dma((3, GROUP)),
        pltpu.SemaphoreType.DMA,
        pltpu.SemaphoreType.DMA,
        pltpu.SemaphoreType.DMA,
        pltpu.SemaphoreType.DMA,
        pltpu.SemaphoreType.DMA,
        dma((parts,)),
        pltpu.SemaphoreType.DMA,
        dma((sides, 2)),
        pltpu.SemaphoreType.DMA,
        dma((parts + 1,)),
        pltpu.SemaphoreType.DMA,
        dma((parts,)),
        dma((2,)),
        dma((parts, 4)),
        pltpu.SemaphoreType.DMA,
        pltpu.SemaphoreType.DMA,
        pltpu.SemaphoreType.DMA,
        pltpu.SemaphoreType.DMA,
        pltpu.SemaphoreType.DMA,
        dma((parts,)),
        pltpu.SemaphoreType.DMA,
        pltpu.SemaphoreType.DMA,
        pltpu.SemaphoreType.DMA,
        dma((CHUNKS,)),
        pltpu.SemaphoreType.DMA,
        pltpu.SemaphoreType.DMA,
        dma((9,)),
    ]
    spec = pl.BlockSpec(memory_space=pl.ANY)
    held = pl.pallas_call(
        functools.partial(kernel, sp_size, tp_size),
        out_shape=(
            pltpu.VMEM((rows, d), BF16),
            pltpu.VMEM((own_rows, d), F32),
            pltpu.VMEM((depth, width), F32),
        ),
        in_specs=[spec] * 9,
        out_specs=(pl.BlockSpec(memory_space=pltpu.VMEM),) * 3,
        scratch_shapes=scratch + sems,
        compiler_params=pltpu.CompilerParams(
            collective_id=0, has_side_effects=True, vmem_limit_bytes=60000 * 1024
        ),
    )(
        *[
            pltpu.with_memory_space_constraint(x, pltpu.HBM)
            for x in (
                target,
                source,
                target_gain.reshape(1, d),
                source_gain.reshape(1, d),
                w_query,
                w_key,
                w_value,
                attended,
                d_attended,
            )
        ]
    )

    return pl.pallas_call(
        store_kernel,
        out_shape=(
            jax.ShapeDtypeStruct((rows, d), BF16),
            jax.ShapeDtypeStruct((own_rows, d), F32),
            jax.ShapeDtypeStruct((depth, width), F32),
        ),
        in_specs=[pl.BlockSpec(memory_space=pltpu.VMEM)] * 3,
        out_specs=(spec,) * 3,
        scratch_shapes=[dma((3,))],
    )(*[pltpu.with_memory_space_constraint(x, pltpu.VMEM) for x in held])


def store_kernel(a, b, c, a_h, b_h, c_h, sem):
    stores = [
        pltpu.make_async_copy(src, dst, sem.at[n])
        for n, (src, dst) in enumerate(((a, a_h), (b, b_h), (c, c_h)))
    ]
    for store in stores:
        store.start()
    for store in stores:
        store.wait()


def solution(mesh):
    return jax.shard_map(
        local,
        mesh=mesh,
        in_specs=(
            P("sp", None),
            P(("sp", "tp"), None),
            P(),
            P(),
            P(None, "tp"),
            P(),
            P(),
            P("sp", "tp"),
            P("sp", "tp"),
        ),
        out_specs=(P("sp", None), P(("sp", "tp"), None), P("sp", "tp")),
        check_vma=False,
    )
```
